32 devices in a mesh: ep: 8 (over z, x), tp: 4 (over y, core).
Axes of the slice: x: 2, y: 2, z: 4, core: 2. Of those that a mesh axis runs over, the one named last changes fastest.
Arguments:
- conv_value: bfloat16 [4096, 2048], P('ep', 'tp'), may hold values from -6 to 6
- conv_gate: bfloat16 [4096, 2048], P('ep', 'tp'), may hold values from -9 to 9
- conv_taps: float32 [31, 2048], P(None, 'tp'), may hold values from -14 to 14
- norm_gain: float32 [2048], P('tp'), may hold values from 0.1 to 1.9
- norm_shift: float32 [2048], P('tp'), may hold values from -3 to 3
- conv_out_weight: bfloat16 [2048, 2048], P(None, 'tp'), may hold values from -0.125 to 0.125
- moe_input: bfloat16 [1024, 2048], P('ep'), may hold values from -6 to 6
- moe_gain: float32 [2048], replicated, may hold values from 0.1 to 1.9
- routes: int32 [1024, 4], P('ep'), may hold values from 0 to 7, all different within a row; in each aligned block of 128 rows (0 to 127, 128 to 255, ...) at most 128 rows name the same one
- route_weights: float32 [1024, 4], P('ep'), may hold values from 0.25 to 1
- expert_gate: bfloat16 [8, 2048, 4096], P('ep', None, 'tp'), may hold values from -0.125 to 0.125
- expert_up: bfloat16 [8, 2048, 4096], P('ep', None, 'tp'), may hold values from -0.125 to 0.125
- expert_down: bfloat16 [8, 4096, 2048], P('ep', None, 'tp'), may hold values from -0.09375 to 0.09375
- shared_gate: bfloat16 [2048, 512], P(None, 'tp'), may hold values from -0.125 to 0.125
- shared_up: bfloat16 [2048, 512], P(None, 'tp'), may hold values from -0.125 to 0.125
- shared_down: bfloat16 [512, 2048], P(None, 'tp'), may hold values from -0.25 to 0.25
Outputs:
- conv_result: bfloat16 [4096, 2048], P('ep', 'tp')
- moe_result: bfloat16 [1024, 2048], P('ep', 'tp')
The draws below stay inside these ranges and needn't reach their ends.
Inputs may be any that keep to these rules, and one draw needn't show every extreme that they name: `routes`: in the rows of one device (aligned blocks of 128 rows) no expert is named by more than 128 rows, a bound that some block reaches; each row names 4 different experts.
All inputs are finite; a program needn't handle non-finite values.
Results may differ from the reference program's by a relative error of at most 0.0068.
Values may be sent and summed in bfloat16 or wider, within the bound.
A program may use at most 64 MiB of HBM per device.

```python
import math
import jax
import jax.numpy as jnp
import numpy as np
from jax import lax

D = 2048
FF = 4096
SHARED_FF = 512
CONV_WIDTH = 31
TOPK = 4
TOKB_DEV = 128
TOK_A = 4096
TOK_B = 1024
EXPERTS = 8
CAP = 128
N_EP = 8


def draw_conv_taps(key, part):
    base_key = jax.random.fold_in(key, 11)
    rough_key = jax.random.fold_in(key, 12)
    channel = jnp.arange(D, dtype=jnp.float32) / D
    base_draw = jnp.clip(jax.random.normal(base_key, (CONV_WIDTH, D), jnp.float32), -5.0, 5.0)
    channel_rise = jnp.exp(jnp.log(4.0) * channel)
    rough_scale = jax.random.uniform(rough_key, (D,), jnp.float32, 0.5, 1.5)
    return base_draw * channel_rise * rough_scale / jnp.sqrt(CONV_WIDTH * 1.0)


def block_scale(stream_key, shape, split, least, high):
    factor_of = 1.0
    for dim, blocks in split:
        draws = jax.random.uniform(jax.random.fold_in(jax.random.fold_in(stream_key, 6), dim), (blocks,), jnp.float32, least / len(split), high / len(split))
        factor_of = factor_of * jnp.repeat(jnp.exp(draws), shape[dim] // blocks).reshape((-1,) + (1,) * (len(shape) - 1 - dim))
    return factor_of


def routed_block(stream_key, own, number, rows, number_of, top, most, skew):
    order = jax.random.permutation(stream_key, number_of)
    packed, common = shares(number_of, rows * top, most, skew, True), shares(number_of, rows * top, most, skew, False)
    places = jnp.arange(number_of)

    def named(sizes, rotation):
        used = int((sizes > 0).sum())
        fixed = max(1, used // 4)
        shifted = fixed + (places - fixed + rotation * (used - fixed)) % max(1, number_of - fixed)
        return jnp.zeros((number_of,), jnp.int32).at[order[jnp.where(places < fixed, places, shifted)]].set(jnp.asarray(sizes, jnp.int32))

    sizes = jnp.where(number % 4 == 0, named(packed, number // 4), named(common, number - number // 4 - 1))
    mixed = jax.random.permutation(jax.random.fold_in(own, 3), number_of)
    giver, receiver = mixed[0:number_of // 2 * 2:2], mixed[1:number_of // 2 * 2:2]
    slack = jnp.minimum(sizes[giver] - 1, most - sizes[receiver]) // 2
    slack = jnp.where((giver == order[0]) | (receiver == order[0]) | (sizes[receiver] == 0), 0, jnp.maximum(slack, 0))
    shifted = jax.random.randint(jax.random.fold_in(own, 4), (number_of // 2,), 0, 1 << 20) % (slack + 1)
    sizes = sizes.at[giver].add(-shifted).at[receiver].add(shifted)
    items = jnp.searchsorted(jnp.cumsum(sizes), jnp.arange(rows * top), side="right").astype(jnp.int32)
    listing = items.reshape(top, rows).T
    listing = listing[jax.random.permutation(jax.random.fold_in(own, 1), rows)]
    rotation = jax.random.randint(jax.random.fold_in(own, 2), (rows, 1), 0, top)
    return jnp.take_along_axis(listing, (jnp.arange(top)[None, :] + rotation) % top, axis=1)


def shares(amount, total, reach, skew, full):
    portions = [(1 << 20) // math.isqrt(rank ** skew) + 1 for rank in range(1, amount + 1)]
    largest = reach if full else min(reach, max(-(-total // amount), total * portions[0] // sum(portions)))
    least = 1 if total - largest >= amount - 1 else 0
    given, surplus = [largest] + [least] * (amount - 1), total - largest - least * (amount - 1)
    while surplus > 0:
        movable = [i for i in range(1, amount) if given[i] < largest] or [i for i in range(1, amount) if given[i] < reach]
        whole, left = sum([portions[i] for i in movable]), surplus
        for i in movable:
            extra = min(reach - given[i], max(1, left * portions[i] // whole), surplus)
            given[i] = given[i] + extra
            surplus = surplus - extra
    return np.array(given)


def noise(rng, shape, width, reach, shards=(), kind=jnp.bfloat16):
    array = jax.random.normal(rng, shape, jnp.float32) * width
    if len(shards) > 0:
        array = block_scale(rng, shape, shards, -0.22, 0.18) * array
    return jnp.clip(array, min=-reach, max=reach).astype(kind)


def setup_inputs(seed: int = 0) -> dict:
    key_list = jax.random.split(jax.random.key(seed), 17)
    conv_value = noise(key_list[0], (TOK_A, D), 1.0, 6.0, ((0, 8), (1, 4)))
    conv_gate = noise(key_list[1], (TOK_A, D), 1.5, 9.0, ((0, 8), (1, 4)))
    conv_taps = draw_conv_taps(jax.random.fold_in(key_list[16], 71), 0)
    norm_gain = jnp.clip(1.0 + 0.18 * jax.random.normal(key_list[3], (D,), jnp.float32), 0.1, 1.9)
    norm_shift = noise(key_list[4], (D,), 0.5, 3.0, ((0, 4),), jnp.float32)
    conv_out_weight = noise(key_list[5], (D, D), D ** -0.5, 0.125, ((1, 4),))
    moe_input = noise(key_list[6], (TOK_B, D), 1.0, 6.0, ((0, 8),))
    moe_gain = jnp.clip(1.0 + 0.18 * jax.random.normal(key_list[7], (D,), jnp.float32), 0.1, 1.9)
    routes_keys = jax.random.split(jax.random.fold_in(key_list[8], 1), TOK_B // TOKB_DEV)
    routes_turns = jax.random.permutation(jax.random.fold_in(key_list[8], 3), TOK_B // TOKB_DEV)
    routes = jax.vmap(lambda own, number: routed_block(jax.random.fold_in(key_list[8], 2), own, number, TOKB_DEV, EXPERTS, TOPK, CAP, 2))(routes_keys, routes_turns).reshape((TOK_B, TOPK))
    route_weights = jnp.clip(0.25 + 0.75 * jax.random.uniform(key_list[9], (TOK_B, TOPK), jnp.float32) ** block_scale(key_list[9], (TOK_B, TOPK), ((0, 8),), -0.2, 0.2), 0.25, 1.0)
    expert_gate = noise(key_list[10], (EXPERTS, D, FF), D ** -0.5, 0.125, ((0, 8), (2, 4)))
    expert_up = noise(key_list[11], (EXPERTS, D, FF), D ** -0.5, 0.125, ((0, 8), (2, 4)))
    expert_down = noise(key_list[12], (EXPERTS, FF, D), FF ** -0.5, 0.09375, ((0, 8), (2, 4)))
    shared_gate = noise(key_list[13], (D, SHARED_FF), D ** -0.5, 0.125, ((1, 4),))
    shared_up = noise(key_list[14], (D, SHARED_FF), D ** -0.5, 0.125, ((1, 4),))
    shared_down = noise(key_list[15], (SHARED_FF, D), SHARED_FF ** -0.5, 0.25, ((1, 4),))
    return {"conv_value": conv_value, "conv_gate": conv_gate, "conv_taps": conv_taps, "norm_gain": norm_gain, "norm_shift": norm_shift, "conv_out_weight": conv_out_weight, "moe_input": moe_input, "moe_gain": moe_gain, "routes": routes, "route_weights": route_weights, "expert_gate": expert_gate, "expert_up": expert_up, "expert_down": expert_down, "shared_gate": shared_gate, "shared_up": shared_up, "shared_down": shared_down}


def reference(conv_value, conv_gate, conv_taps, norm_gain, norm_shift, conv_out_weight, moe_input, moe_gain, routes, route_weights, expert_gate, expert_up, expert_down, shared_gate, shared_up, shared_down):
    glu_rows = (conv_value.astype(jnp.float32) * jax.nn.sigmoid(conv_gate.astype(jnp.float32))).astype(jnp.bfloat16)
    padded = jnp.concatenate([jnp.zeros((CONV_WIDTH - 1, D), jnp.bfloat16), glu_rows], axis=0)
    filtered = jnp.zeros((TOK_A, D), jnp.float32)
    for offset in range(CONV_WIDTH):
        filtered = filtered + conv_taps[offset] * padded[offset:offset + TOK_A].astype(jnp.float32)
    row_mean = lax.optimization_barrier(jnp.mean(filtered, axis=1, keepdims=True))
    row_square = lax.optimization_barrier(jnp.mean(filtered * filtered, axis=1, keepdims=True))
    scaled = (filtered - row_mean) * lax.rsqrt(row_square - row_mean * row_mean + 1e-05)
    conv_hidden = jax.nn.silu(scaled * norm_gain + norm_shift).astype(jnp.bfloat16)
    conv_result = jnp.dot(conv_hidden, conv_out_weight, preferred_element_type=jnp.float32).astype(jnp.bfloat16)
    inputs = moe_input.astype(jnp.float32)
    normed = (inputs * lax.rsqrt(lax.optimization_barrier(jnp.mean(inputs * inputs, axis=1, keepdims=True)) + 1e-06) * moe_gain).astype(jnp.bfloat16)
    flat_expert = routes.reshape(-1).astype(jnp.int32)
    owner_row = (jnp.arange(TOK_B * TOPK, dtype=jnp.int32) // TOPK).astype(jnp.int32)
    sort_order = jnp.argsort(flat_expert, stable=True).astype(jnp.int32)
    sorted_owner = owner_row[sort_order]
    sorted_weight = route_weights.reshape(-1)[sort_order]
    counts = lax.optimization_barrier(jnp.sum((flat_expert[:, None] == jnp.arange(EXPERTS, dtype=jnp.int32)[None, :]).astype(jnp.int32), axis=0))
    starts = (jnp.cumsum(counts) - counts).astype(jnp.int32)
    slot_limit = N_EP * CAP
    pad_owner = jnp.concatenate([sorted_owner, jnp.zeros((slot_limit,), jnp.int32)])
    pad_weight = jnp.concatenate([sorted_weight, jnp.zeros((slot_limit,), jnp.float32)])

    def one_expert(running, expert_id):
        first_row = starts[expert_id]
        row_ids = lax.dynamic_slice_in_dim(pad_owner, first_row, slot_limit)
        weight = lax.dynamic_slice_in_dim(pad_weight, first_row, slot_limit)
        live_mask = (jnp.arange(slot_limit, dtype=jnp.int32) < counts[expert_id]).astype(jnp.float32)
        picked_rows = normed[row_ids]
        hidden = (jax.nn.silu(jnp.dot(picked_rows, expert_gate[expert_id], preferred_element_type=jnp.float32)) * jnp.dot(picked_rows, expert_up[expert_id], preferred_element_type=jnp.float32)).astype(jnp.bfloat16)
        expert_rows = jnp.dot(hidden, expert_down[expert_id], preferred_element_type=jnp.float32).astype(jnp.bfloat16)
        expert_rows = lax.optimization_barrier(expert_rows).astype(jnp.float32)
        return (running.at[row_ids].add(expert_rows * (weight * live_mask)[:, None]), None)
    routed, _ = lax.scan(one_expert, jnp.zeros((TOK_B, D), jnp.float32), jnp.arange(EXPERTS, dtype=jnp.int32))
    shared_hidden = (jax.nn.silu(jnp.dot(normed, shared_gate, preferred_element_type=jnp.float32)) * jnp.dot(normed, shared_up, preferred_element_type=jnp.float32)).astype(jnp.bfloat16)
    shared_sum = jnp.dot(shared_hidden, shared_down, preferred_element_type=jnp.float32)
    moe_result = (routed + shared_sum).astype(jnp.bfloat16)
    return (conv_result, moe_result)
```

```python
import functools
import types

import jax
import jax.numpy as jnp
from jax import lax
from jax.experimental import pallas as pl
from jax.experimental.pallas import tpu as pltpu
from jax.sharding import PartitionSpec as P

MESH = pl.DeviceIdType.MESH
CHUNK = 64
SPAN = 128
PIECES = 4
TP = 4


def from_behind(value, axis, steps):
    count = lax.axis_size(axis)
    initial, last = (max(0, -steps), min(count, count - steps))
    return lax.ppermute(value, axis, [(source, source + steps) for source in range(initial, last)])


def silu(v):
    return v / (1.0 + jnp.exp(-v))


def phase(step):
    def run(*args, **settings):
        with jax.named_scope(step.__name__):
            return step(*args, **settings)

    return run


def layer_kernel(depth, names, *refs):
    r = types.SimpleNamespace(**dict(zip(names, refs, strict=True)))
    e = lax.axis_index("ep")
    q = lax.axis_index("tp")
    z, x = e // 2, e % 2
    y, c = q // 2, q % 2
    side = y * 2 + (1 - c)
    far = (1 - y) * 2 + c
    opposite = (1 - y) * 2 + (1 - c)
    sister, across, beside = (e, side), (e, far), (z * 2 + (1 - x), q)
    blocks = 2 * depth
    bf, f32 = jnp.bfloat16, jnp.float32

    tokens, hidden, chidden, shidden, padded = r.tokens, r.hidden, r.chidden, r.shidden, r.padded
    rows, width = r.x_in.shape
    half = width // 2
    units = r.gate.shape[1]
    rows_a, channels = r.value.shape
    tap_count, edge = r.taps.shape[0], r.halo.shape[0]
    lead = edge - (tap_count - 1)
    chunks = rows_a // CHUNK
    spans = rows_a // SPAN
    everything = slice(0, rows)

    upper = z // 2
    inside = (z + upper) % 2
    inner, outer = inside == 1, inside == 0
    mate = z + 1 - 2 * (z % 2)
    facing = depth - 1 - z
    origin = [z, mate, 2 - upper, 3 - 3 * upper]
    back = [0, 1, 3 - inside, 3 - inside]

    def place(b):
        return origin[b // 2] * 2 + (x if b % 2 == 0 else 1 - x)

    def slab(size, parts, i):
        return slice(i * size // parts, (i + 1) * size // parts)

    def dot(a, b):
        return jnp.dot(a, b, preferred_element_type=f32)

    def copy(src, dst, send, recv, device):
        return pltpu.make_async_remote_copy(
            src_ref=src, dst_ref=dst, send_sem=send.at[0], recv_sem=recv, device_id=device, device_id_type=MESH
        )

    def launch(*args):
        copy(*args).start()

    def landed(like, recv):
        copy(like, like, r.e_send, recv, beside).wait_recv()

    def gone(like, send):
        copy(like, like, send, r.e_recv.at[0], beside).wait_send()

    loads = []

    def load(*pairs):
        sem = r.load_sem.at[len(loads)]
        loads.append(sem)
        for src, dst in pairs:
            pltpu.make_async_copy(src, dst, sem).start()
        return sem

    def loaded(sem, src, dst):
        pltpu.make_async_copy(src, dst, sem).wait()

    gate_cols = [slab(units, PIECES, t) for t in range(PIECES)]
    tail_rows, other_rows = slice(rows_a - CHUNK, rows_a), slice(0, rows_a - CHUNK)
    x_sem = load((r.x_hbm, r.x_in))
    moe_gain_sem = load((r.moe_gain_hbm, r.moe_gain))
    tail_sems = [
        load((r.value_hbm.at[tail_rows], r.value.at[tail_rows])),
        load((r.cgate_hbm.at[tail_rows], r.cgate.at[tail_rows])),
    ]
    gate_sems = [
        load((r.gate_hbm.at[0, :, cols], r.gate.at[:, cols]), (r.up_hbm.at[0, :, cols], r.up.at[:, cols]))
        for cols in gate_cols
    ]
    rest = [
        (r.value_hbm.at[other_rows], r.value.at[other_rows]),
        (r.cgate_hbm.at[other_rows], r.cgate.at[other_rows]),
        (r.sgate_hbm, r.sgate),
        (r.sup_hbm, r.sup),
        (r.taps_hbm, r.taps),
        (r.gain_hbm, r.gain),
        (r.shift_hbm, r.shift),
        (r.routes_hbm, r.routes),
        (r.route_weights_hbm, r.route_weights),
    ]
    rest_sems = [load(pair) for pair in rest]

    peers = [(place(b), q) for b in range(1, blocks)]
    peers += [(e, (q + k) % TP) for k in range(1, TP)]
    barrier = pltpu.get_barrier_semaphore()
    for peer in peers:
        pl.semaphore_signal(barrier, inc=1, device_id=peer, device_id_type=MESH)

    def chunk_of(i):
        return pl.multiple_of(i * CHUNK, CHUNK)

    def glu(i, carry):
        at = pl.ds(chunk_of(i), CHUNK)
        gated = r.value[at, :].astype(f32) * (1.0 / (1.0 + jnp.exp(-r.cgate[at, :].astype(f32))))
        padded[pl.ds(pl.multiple_of(i * CHUNK + edge, 8), CHUNK), :] = gated.astype(bf).astype(f32)
        return carry

    lane = lax.broadcasted_iota(jnp.int32, (CHUNK, 128), 1)

    def convolve(i, carry):
        start = chunk_of(i)
        at = pl.ds(start, CHUNK)
        sums, squares = jnp.zeros((CHUNK, 128), f32), jnp.zeros((CHUNK, 128), f32)
        for column in range(0, channels, 128):
            cols = slice(column, column + 128)
            window = padded[pl.ds(start, CHUNK + edge), cols]
            total = jnp.zeros((CHUNK, 128), f32)
            for b in range(8):
                size = CHUNK + (8 if b else 0)
                part = None
                for a in range(edge // 8 + 1):
                    j = 8 * a + b - lead
                    if 0 <= j < tap_count:
                        term = r.taps[j : j + 1, cols] * window[8 * a : 8 * a + size]
                        part = term if part is None else part + term
                if b:
                    part = pltpu.roll(part, size - b, 0)[:CHUNK]
                total = total + part
            r.filtered[at, cols] = total
            sums = sums + total
            squares = squares + total * total
        row_sum = jnp.sum(sums, axis=1, keepdims=True)
        row_squares = jnp.sum(squares, axis=1, keepdims=True)
        r.stats[at, :] = jnp.where(lane == 0, row_sum, jnp.where(lane == 1, row_squares, 0.0))
        return carry

    @phase
    def conv(first_chunk, last_chunk):
        lax.fori_loop(first_chunk, last_chunk, convolve, 0)

    @phase
    def halo():
        landed(r.halo, r.e_recv.at[0])
        padded[0:edge, :] = jnp.where(e == 0, 0.0, r.halo[...].astype(f32))

    @phase
    def send_stats():
        turned = r.stats[...].T
        lines = [turned[k : k + 1, slab(rows_a, spans, j)] for k in range(2) for j in range(spans)]
        r.rowsums[q] = jnp.concatenate(lines, axis=0)
        mine = r.rowsums.at[q]
        for k in range(1, TP):
            launch(mine, mine, r.m_send, r.m_recv.at[0], (e, (q + k) % TP))

    @phase
    def normalise():
        landed(r.rowsums.at[0 : TP - 1], r.m_recv.at[0])
        whole = (r.rowsums[0] + r.rowsums[1] + r.rowsums[2] + r.rowsums[3]) / (channels * TP)
        turned = jnp.concatenate([whole, jnp.zeros((SPAN - 2 * spans, SPAN), f32)], axis=0).T
        r.stats[0:SPAN, :] = turned
        for j in range(spans):

            def scale(i, carry):
                here = chunk_of(i)
                at = pl.ds(pl.multiple_of(here + j * SPAN, CHUNK), CHUNK)
                both = r.stats[pl.ds(here, CHUNK), :]
                mean, square = both[:, j : j + 1], both[:, spans + j : spans + j + 1]
                scaled = (r.filtered[at, :] - mean) * lax.rsqrt(square - mean * mean + 1e-05)
                chidden[q, at, :] = silu(scaled * r.gain[...] + r.shift[...]).astype(bf)
                return carry

            lax.fori_loop(0, SPAN // CHUNK, scale, 0)

    def send_conv(j):
        block = chidden.at[q, slab(rows_a, spans, j)]
        launch(block, block, r.c_send, r.ca_recv.at[j], across)
        launch(block, block, r.c_send, r.cs_recv.at[0], sister)

    @phase
    def relay_conv(j):
        block = chidden.at[far, slab(rows_a, spans, j)]
        landed(block, r.ca_recv.at[j])
        launch(block, block, r.c_send, r.cf_recv.at[j], sister)

    def conv_part(j, k):
        at = pl.ds(pl.multiple_of(k * channels, channels), channels)
        return dot(chidden[k, slab(rows_a, spans, j), :], r.cweight[at, :])

    @phase
    def project(j, base=None):
        at = slab(rows_a, spans, j)
        total = conv_part(j, q) + conv_part(j, side) + conv_part(j, far) if base is None else base + conv_part(j, far)
        landed(chidden.at[opposite, at], r.cf_recv.at[j])
        r.conv_done[at, :] = (total + conv_part(j, opposite)).astype(bf)
        pltpu.make_async_copy(r.conv_done.at[at], r.conv_out.at[at], out_sem).start()

    def towards(src, slot, z_to):
        return copy(src, tokens.at[2 * slot, c], r.z_send, r.z_recv.at[slot - 1], (z_to * 2 + x, q))

    halves = [slab(rows, 2, i) for i in range(2)]

    @phase
    def pass_on(b, i=0, part=everything, condition=None):
        block = tokens.at[b, c, part]

        def along():
            (towards(block, 3, facing) if b == 2 else towards(block, b // 2, mate)).start()

        def act():
            landed(block, r.z_recv.at[b // 2 - 1] if b % 2 == 0 else r.t_recv.at[b // 2 + (1 if b > 1 else i)])
            if b % 2 == 0:
                if condition is inner:
                    along()
                elif condition is None:
                    pl.when(inner)(along)
                launch(block, tokens.at[b + 1, c, part], r.t_send, r.t_recv.at[b // 2 + 1], beside)
            launch(block, block, r.f_send, r.f_recv.at[b if b > 1 else i], sister)

        if condition is None:
            act()
        else:
            pl.when(condition)(act)

    @phase
    def swap_wait(b, i=0, part=everything):
        landed(tokens.at[b, 1 - c, part], r.f_recv.at[b if b > 1 else i])

    @phase
    def first(b, part, cols):
        def product(weight):
            return sum(dot(tokens[b, h, part, :], weight[h * half : (h + 1) * half, cols]) for h in range(2))

        hidden[b, q, part, cols] = (silu(product(r.gate)) * product(r.up)).astype(bf)
        block = hidden.at[b, q, part, cols]
        launch(block, block, r.h_send, r.y_recv.at[b], across)
        launch(block, block, r.h_send, r.p_recv.at[b], sister)

    def block_first(b):
        for t in range(2):
            first(b, everything, slab(units, 2, t))

    @phase
    def relay(b):
        block = hidden.at[b, far]
        landed(block, r.y_recv.at[b])
        launch(block, block, r.h_send, r.p_recv.at[b], sister)

    @phase
    def second_wait(b):
        landed(hidden.at[b, 0:2], r.p_recv.at[b])

    @phase
    def second(b):
        total = sum(dot(hidden[b, k], r.down[k * units : (k + 1) * units, :]) for k in range(TP))
        if b == 0:
            r.returned[0] = total.astype(bf)
        else:
            r.outgoing[b] = total.astype(bf)
            there = 2 * back[b // 2] + b % 2
            launch(r.outgoing.at[b], r.returned.at[there], r.r_send, r.r_recv.at[0], (place(b), q))

    def finish(b):
        second_wait(b)
        second(b)

    @phase
    def norm():
        loaded(x_sem, r.x_hbm, r.x_in)
        loaded(moe_gain_sem, r.moe_gain_hbm, r.moe_gain)
        for i in range(rows // 16):
            at = slice(i * 16, i * 16 + 16)
            v = r.x_in[at, :].astype(f32)
            scale = lax.rsqrt(jnp.mean(v * v, axis=1, keepdims=True) + 1e-06)
            normed = (v * scale * r.moe_gain[...]).astype(bf)
            tokens[0, 0, at, :] = normed[:, :half]
            tokens[0, 1, at, :] = normed[:, half:]

    @phase
    def tail_glu():
        loaded(tail_sems[0], r.value_hbm.at[tail_rows], r.value.at[tail_rows])
        loaded(tail_sems[1], r.cgate_hbm.at[tail_rows], r.cgate.at[tail_rows])
        glu(chunks - 1, 0)
        r.tail[...] = padded[rows_a:, :].astype(bf)

    @phase
    def meet():
        pl.semaphore_wait(barrier, len(peers))

    norm()
    tail_glu()
    meet()
    for i, part in enumerate(halves):
        launch(tokens.at[0, c, part], tokens.at[1, c, part], r.t_send, r.t_recv.at[i], beside)
    towards(tokens.at[0, c], 1, mate).start()
    pl.when(inner)(lambda: towards(tokens.at[0, c], 2, facing).start())
    launch(r.tail, r.halo, r.e_send, r.e_recv.at[0], ((e + 1) % blocks, q))

    for t, cols in enumerate(gate_cols):
        both = slab(units, PIECES // 2, 0)
        loaded(gate_sems[t], r.gate_hbm.at[0, :, both], r.gate.at[:, both])
        first(0, everything, cols)

    cweight_sem = load((r.cweight_hbm, r.cweight))
    down_sem = load((r.down_hbm.at[0], r.down))
    sdown_sem = load((r.sdown_hbm, r.sdown))
    out_sem = r.load_sem.at[len(loads)]

    @phase
    def glu_rest():
        for sem, pair in zip(rest_sems, rest, strict=True):
            loaded(sem, *pair)
        lax.fori_loop(0, chunks - 1, glu, 0)

    @phase
    def shared():
        def product(weight):
            return sum(dot(tokens[0, h], weight[h * half : (h + 1) * half, :]) for h in range(2))

        shidden[q] = (silu(product(r.sgate)) * product(r.sup)).astype(bf)
        launch(shidden.at[q], shidden.at[q], r.s_send, r.s_recv.at[0], across)
        launch(shidden.at[q], shidden.at[q], r.s_send, r.s_recv.at[1], sister)

    @phase
    def relay_shared():
        landed(shidden.at[far], r.s_recv.at[0])
        launch(shidden.at[far], shidden.at[far], r.s_send, r.s_recv.at[1], sister)

    @phase
    def shared_down():
        loaded(sdown_sem, r.sdown_hbm, r.sdown)
        landed(shidden.at[0:2], r.s_recv.at[1])
        share = shidden.shape[2]
        r.shared_sum[...] = sum(dot(shidden[k], r.sdown[k * share : (k + 1) * share, :]) for k in range(TP))

    @phase
    def combine():
        landed(r.returned.at[1:blocks], r.r_recv.at[0])
        routes, route_weights = r.routes[...], r.route_weights[...]
        lines = []
        for b in range(blocks):
            lines.append(jnp.sum(jnp.where(routes == place(b), route_weights, 0.0), axis=0, keepdims=True))
        lines.append(jnp.zeros((128 - blocks, rows), f32))
        weights = jnp.concatenate(lines, axis=0).T
        moe_sum = r.shared_sum[...]
        for b in range(blocks):
            moe_sum = moe_sum + weights[:, b : b + 1] * r.returned[b].astype(f32)
        r.done[...] = moe_sum.astype(bf)
        pltpu.make_async_copy(r.done, r.out, x_sem).start()

    glu_rest()
    shared()
    conv(1, 4)
    pass_on(1, 0, halves[0])
    conv(4, 5)
    swap_wait(1, 0, halves[0])
    for t in range(2):
        first(1, halves[0], slab(units, 2, t))
    pass_on(1, 1, halves[1])
    pass_on(2)
    pass_on(4, condition=inner)
    conv(5, 6)
    swap_wait(1, 1, halves[1])
    for t in range(2):
        first(1, halves[1], slab(units, 2, t))
    swap_wait(2)
    block_first(2)
    relay(0)
    conv(6, 7)
    pass_on(4, condition=outer)
    conv(7, chunks)
    halo()
    conv(0, 1)
    send_stats()
    pass_on(6, condition=inner)
    pass_on(3)
    swap_wait(4)
    block_first(4)
    relay(1)
    relay_shared()
    loaded(down_sem, r.down_hbm.at[0], r.down)
    finish(0)
    pass_on(6, condition=outer)
    pass_on(5)
    swap_wait(6)
    block_first(6)
    relay(2)
    finish(1)
    swap_wait(5)
    block_first(5)
    finish(2)
    normalise()
    pass_on(7)
    swap_wait(7)
    block_first(7)
    swap_wait(3)
    block_first(3)
    for j in range(spans):
        send_conv(j)
    for b in (4, 6, 5, 7, 3):
        relay(b)
        if b == 3:
            shared_down()
        finish(b)
    loaded(cweight_sem, r.cweight_hbm, r.cweight)
    landed(chidden.at[side], r.cs_recv.at[0])
    last = spans - 1
    for j in range(last):
        relay_conv(j)
        if j:
            project(j - 1)
    combine()
    r.partial[...] = conv_part(last, q) + conv_part(last, side)
    project(last - 1)
    relay_conv(last)
    project(last, r.partial[...])

    @phase
    def drain():
        gone(hidden.at[:, 0:3], r.h_send)
        gone(r.outgoing.at[1:blocks], r.r_send)
        gone(tokens.at[0:depth, c], r.t_send)
        gone(tokens.at[1:blocks, c], r.f_send)
        pl.when(inner)(lambda: gone(tokens.at[0:5, c], r.z_send))
        pl.when(outer)(lambda: gone(tokens.at[0, c], r.z_send))
        gone(r.rowsums.at[0 : TP - 1], r.m_send)
        gone(shidden.at[0:3], r.s_send)
        gone(chidden.at[0:3], r.c_send)
        gone(r.tail, r.e_send)
        pltpu.make_async_copy(r.done, r.out, x_sem).wait()
        pltpu.make_async_copy(r.conv_done, r.conv_out, out_sem).wait()

    drain()


def hand_out(conv_done, done, conv_out, out, conv_held, held, sems):
    parts = [(conv_done, conv_held, conv_out, slice(at, at + SPAN)) for at in range(0, conv_done.shape[0], SPAN)]
    parts.append((done, held, out, slice(0, done.shape[0])))
    ins = [pltpu.make_async_copy(src.at[at], mid.at[at], sems.at[0, i]) for i, (src, mid, _, at) in enumerate(parts)]
    outs = [pltpu.make_async_copy(mid.at[at], dst.at[at], sems.at[1, i]) for i, (_, mid, dst, at) in enumerate(parts)]
    for cp in ins:
        cp.start()
    for cp, then in zip(ins, outs):
        cp.wait()
        then.start()
    for cp in outs:
        cp.wait()


def fused(
    conv, moe_input, moe_gain, routes, route_weights, expert_gate, expert_up, expert_down, shared_gate, shared_up, shared_down
):
    value, cgate, taps, gain, shift, cweight = conv
    rows_a, channels = value.shape
    spans = rows_a // SPAN
    edge = -(-(taps.shape[0] - 1) // 8) * 8
    rows, width = moe_input.shape
    depth = lax.axis_size("ep") // 2
    blocks = 2 * depth
    units, columns = expert_gate.shape[2], expert_down.shape[2]
    bf, f32 = jnp.bfloat16, jnp.float32
    hbm = pl.BlockSpec(memory_space=pl.ANY)

    def held(like):
        return pltpu.VMEM(like.shape, like.dtype)

    def dma(*shape):
        return pltpu.SemaphoreType.DMA(shape)

    gain, shift, moe_gain = gain.reshape(1, -1), shift.reshape(1, -1), moe_gain.reshape(1, -1)
    routes, route_weights = routes.T, route_weights.T
    operands = dict(
        x_hbm=moe_input,
        gate_hbm=expert_gate,
        up_hbm=expert_up,
        down_hbm=expert_down,
        sgate_hbm=shared_gate,
        sup_hbm=shared_up,
        sdown_hbm=shared_down,
        value_hbm=value,
        cgate_hbm=cgate,
        cweight_hbm=cweight,
        taps_hbm=taps,
        gain_hbm=gain,
        shift_hbm=shift,
        moe_gain_hbm=moe_gain,
        routes_hbm=routes,
        route_weights_hbm=route_weights,
    )
    outputs = dict(
        conv_out=jax.ShapeDtypeStruct((rows_a, cweight.shape[1]), bf),
        out=jax.ShapeDtypeStruct((rows, columns), bf),
    )
    scratch = dict(
        x_in=held(moe_input),
        sgate=held(shared_gate),
        sup=held(shared_up),
        sdown=held(shared_down),
        value=held(value),
        cgate=held(cgate),
        cweight=held(cweight),
        taps=held(taps),
        gain=held(gain),
        shift=held(shift),
        moe_gain=held(moe_gain),
        routes=held(routes),
        route_weights=held(route_weights),
        gate=pltpu.VMEM(expert_gate.shape[1:], bf),
        up=pltpu.VMEM(expert_up.shape[1:], bf),
        down=pltpu.VMEM(expert_down.shape[1:], bf),
        padded=pltpu.VMEM((rows_a + edge, channels), f32),
        filtered=pltpu.VMEM((rows_a, channels), f32),
        stats=pltpu.VMEM((rows_a, 128), f32),
        tail=pltpu.VMEM((edge, channels), bf),
        halo=pltpu.VMEM((edge, channels), bf),
        rowsums=pltpu.VMEM((TP, 2 * spans, SPAN), f32),
        chidden=pltpu.VMEM((TP, rows_a, channels), bf),
        partial=pltpu.VMEM((SPAN, cweight.shape[1]), f32),
        tokens=pltpu.VMEM((blocks, 2, rows, width // 2), bf),
        hidden=pltpu.VMEM((blocks, TP, rows, units), bf),
        returned=pltpu.VMEM((blocks, rows, columns), bf),
        outgoing=pltpu.VMEM((blocks, rows, columns), bf),
        shidden=pltpu.VMEM((TP, rows, shared_gate.shape[1]), bf),
        shared_sum=pltpu.VMEM((rows, columns), f32),
        conv_done=held(outputs["conv_out"]),
        done=held(outputs["out"]),
        load_sem=dma(PIECES + 17),
        e_send=dma(1),
        e_recv=dma(1),
        t_send=dma(1),
        t_recv=dma(depth + 1),
        f_send=dma(1),
        f_recv=dma(blocks),
        z_send=dma(1),
        z_recv=dma(depth - 1),
        h_send=dma(1),
        y_recv=dma(blocks),
        p_recv=dma(blocks),
        r_send=dma(1),
        r_recv=dma(1),
        m_send=dma(1),
        m_recv=dma(1),
        s_send=dma(1),
        s_recv=dma(2),
        c_send=dma(1),
        ca_recv=dma(spans),
        cs_recv=dma(1),
        cf_recv=dma(spans),
    )
    flops = 2 * blocks * rows * (2 * width * units + 4 * units * columns)
    results = pl.pallas_call(
        functools.partial(layer_kernel, depth, (*operands, *outputs, *scratch)),
        out_shape=tuple(outputs.values()),
        in_specs=[hbm] * len(operands),
        out_specs=(hbm, hbm),
        scratch_shapes=list(scratch.values()),
        compiler_params=pltpu.CompilerParams(
            collective_id=0, has_side_effects=True, vmem_limit_bytes=56 * 1024 * 1024
        ),
        cost_estimate=pl.CostEstimate(flops=flops * 2, bytes_accessed=40_000_000, transcendentals=0),
    )(*operands.values())
    return pl.pallas_call(
        hand_out,
        out_shape=tuple(outputs.values()),
        in_specs=[hbm, hbm],
        out_specs=(hbm, hbm),
        scratch_shapes=[held(out) for out in outputs.values()] + [dma(2, spans + 1)],
        compiler_params=pltpu.CompilerParams(vmem_limit_bytes=56 * 1024 * 1024),
    )(*results)


def moe_general(normed, routes, route_weights, expert_gate, expert_up, expert_down, shared_gate, shared_up, shared_down):
    rows_b, per_row = routes.shape
    model_width = normed.shape[1]
    groups = lax.axis_size("ep")
    capacity = 2 * rows_b * per_row // groups
    flat_expert = routes.reshape(-1)
    owner_row = jnp.arange(rows_b * per_row, dtype=jnp.int32) // per_row
    expert_hits = (flat_expert[:, None] == jnp.arange(groups, dtype=jnp.int32)[None, :]).astype(
        jnp.int32
    )
    slot_rank = jnp.sum((jnp.cumsum(expert_hits, axis=0) - expert_hits) * expert_hits, axis=1)
    slot_index = flat_expert * capacity + slot_rank
    outgoing = (
        jnp.zeros((groups * capacity, model_width), jnp.bfloat16)
        .at[slot_index]
        .set(normed[owner_row])
    )
    outgoing = outgoing.reshape(groups, capacity, model_width)
    slot_share = capacity // lax.axis_size("tp")
    own_slots = lax.dynamic_slice_in_dim(outgoing, lax.axis_index("tp") * slot_share, slot_share, 1)
    partial_rows = lax.all_to_all(own_slots, "ep", split_axis=0, concat_axis=0, tiled=True)
    arrived = lax.all_gather(partial_rows, "tp", axis=1, tiled=True)
    arrived_rows = arrived.reshape(groups * capacity, model_width)
    gate_value = jnp.dot(arrived_rows, expert_gate[0], preferred_element_type=jnp.float32)
    upward = jnp.dot(arrived_rows, expert_up[0], preferred_element_type=jnp.float32)
    expert_hidden = (jax.nn.silu(gate_value) * upward).astype(jnp.bfloat16)
    shared_hidden = (
        jax.nn.silu(jnp.dot(normed, shared_gate, preferred_element_type=jnp.float32))
        * jnp.dot(normed, shared_up, preferred_element_type=jnp.float32)
    ).astype(jnp.bfloat16)
    columns = expert_down.shape[2]
    routed_sum = jnp.dot(
        lax.all_gather(expert_hidden, "tp", axis=1, tiled=True),
        expert_down[0],
        preferred_element_type=jnp.float32,
    )
    shared_sum = jnp.dot(
        lax.all_gather(shared_hidden, "tp", axis=1, tiled=True),
        shared_down,
        preferred_element_type=jnp.float32,
    )
    expert_out = routed_sum.astype(jnp.bfloat16).reshape(groups, capacity, columns)
    returned = lax.all_to_all(expert_out, "ep", split_axis=0, concat_axis=0, tiled=True).reshape(
        groups * capacity, columns
    )
    picked = returned[slot_index].astype(jnp.float32) * route_weights.reshape(-1)[:, None]
    moe_sum = jnp.sum(picked.reshape(rows_b, per_row, columns), axis=1) + shared_sum
    return moe_sum.astype(jnp.bfloat16)


def conv_general(conv_value, conv_gate, conv_taps, norm_gain, norm_shift, conv_out_weight):
    tap_count = conv_taps.shape[0]
    rows_a = conv_value.shape[0]
    glu_rows = (
        conv_value.astype(jnp.float32) * jax.nn.sigmoid(conv_gate.astype(jnp.float32))
    ).astype(jnp.bfloat16)
    before = from_behind(glu_rows[rows_a - (tap_count - 1) :], "ep", 1)
    padded = jnp.concatenate([before, glu_rows], axis=0)
    filtered = jnp.zeros(glu_rows.shape, jnp.float32)
    for offset in range(tap_count):
        filtered = filtered + conv_taps[offset] * padded[offset : offset + rows_a].astype(
            jnp.float32
        )
    row_total, squares = lax.psum(
        (jnp.sum(filtered, axis=1), jnp.sum(filtered * filtered, axis=1)), "tp"
    )
    channels = conv_out_weight.shape[0]
    row_mean = row_total / channels
    row_square = squares / channels
    scaled = (filtered - row_mean[:, None]) * lax.rsqrt(row_square - row_mean * row_mean + 1e-05)[
        :, None
    ]
    conv_hidden = jax.nn.silu(scaled * norm_gain + norm_shift).astype(jnp.bfloat16)
    conv_sum = jnp.dot(
        lax.all_gather(conv_hidden, "tp", axis=1, tiled=True),
        conv_out_weight,
        preferred_element_type=jnp.float32,
    )
    return conv_sum.astype(jnp.bfloat16)


def body(
    conv_value,
    conv_gate,
    conv_taps,
    norm_gain,
    norm_shift,
    conv_out_weight,
    moe_input,
    moe_gain,
    routes,
    route_weights,
    expert_gate,
    expert_up,
    expert_down,
    shared_gate,
    shared_up,
    shared_down,
):
    conv = (conv_value, conv_gate, conv_taps, norm_gain, norm_shift, conv_out_weight)
    moe = (routes, route_weights, expert_gate, expert_up, expert_down, shared_gate, shared_up, shared_down)
    if lax.axis_size("tp") == TP and lax.axis_size("ep") == 8 and moe_input.shape[0] == 128:
        return fused(conv, moe_input, moe_gain, *moe)
    inputs = moe_input.astype(jnp.float32)
    normed = (
        inputs * lax.rsqrt(jnp.mean(inputs * inputs, axis=1, keepdims=True) + 1e-06) * moe_gain
    ).astype(jnp.bfloat16)
    return (conv_general(*conv), moe_general(normed, *moe))


def solution(mesh):
    return jax.shard_map(
        body,
        mesh=mesh,
        in_specs=(
            P("ep", "tp"),
            P("ep", "tp"),
            P(None, "tp"),
            P("tp"),
            P("tp"),
            P(None, "tp"),
            P("ep", None),
            P(),
            P("ep", None),
            P("ep", None),
            P("ep", None, "tp"),
            P("ep", None, "tp"),
            P("ep", None, "tp"),
            P(None, "tp"),
            P(None, "tp"),
            P(None, "tp"),
        ),
        out_specs=(P("ep", "tp"), P("ep", "tp")),
        check_vma=False,
    )
```

```python
import functools
import types

import jax
import jax.numpy as jnp
from jax import lax
from jax.experimental import pallas as pl
from jax.experimental.pallas import tpu as pltpu
from jax.sharding import PartitionSpec as P

MESH = pl.DeviceIdType.MESH
CHUNK = 64
SPAN = 128
PIECES = 4
TP = 4


def from_behind(value, axis, steps):
    count = lax.axis_size(axis)
    initial, last = (max(0, -steps), min(count, count - steps))
    return lax.ppermute(value, axis, [(source, source + steps) for source in range(initial, last)])


def silu(v):
    return v / (1.0 + jnp.exp(-v))


def phase(step):
    def run(*args, **settings):
        with jax.named_scope(step.__name__):
            return step(*args, **settings)

    return run


def layer_kernel(depth, names, *refs):
    r = types.SimpleNamespace(**dict(zip(names, refs, strict=True)))
    e = lax.axis_index("ep")
    q = lax.axis_index("tp")
    z, x = e // 2, e % 2
    y, c = q // 2, q % 2
    side = y * 2 + (1 - c)
    far = (1 - y) * 2 + c
    opposite = (1 - y) * 2 + (1 - c)
    sister, across, beside = (e, side), (e, far), (z * 2 + (1 - x), q)
    blocks = 2 * depth
    bf, f32 = jnp.bfloat16, jnp.float32

    tokens, hidden, chidden, shidden, padded = r.tokens, r.hidden, r.chidden, r.shidden, r.padded
    rows, width = r.x_in.shape
    half = width // 2
    units = r.gate.shape[1]
    rows_a, channels = r.value.shape
    tap_count, edge = r.taps.shape[0], r.halo.shape[0]
    lead = edge - (tap_count - 1)
    chunks = rows_a // CHUNK
    spans = rows_a // SPAN
    everything = slice(0, rows)

    upper = z // 2
    inside = (z + upper) % 2
    inner, outer = inside == 1, inside == 0
    mate = z + 1 - 2 * (z % 2)
    facing = depth - 1 - z
    origin = [z, mate, 2 - upper, 3 - 3 * upper]
    back = [0, 1, 3 - inside, 3 - inside]

    def place(b):
        return origin[b // 2] * 2 + (x if b % 2 == 0 else 1 - x)

    def slab(size, parts, i):
        return slice(i * size // parts, (i + 1) * size // parts)

    def dot(a, b):
        return jnp.dot(a, b, preferred_element_type=f32)

    def copy(src, dst, send, recv, device):
        return pltpu.make_async_remote_copy(
            src_ref=src, dst_ref=dst, send_sem=send.at[0], recv_sem=recv, device_id=device, device_id_type=MESH
        )

    def launch(*args):
        copy(*args).start()

    def landed(like, recv):
        copy(like, like, r.e_send, recv, beside).wait_recv()

    def gone(like, send):
        copy(like, like, send, r.e_recv.at[0], beside).wait_send()

    loads = []

    def load(*pairs):
        sem = r.load_sem.at[len(loads)]
        loads.append(sem)
        for src, dst in pairs:
            pltpu.make_async_copy(src, dst, sem).start()
        return sem

    def loaded(sem, src, dst):
        pltpu.make_async_copy(src, dst, sem).wait()

    gate_cols = [slab(units, PIECES, t) for t in range(PIECES)]
    tail_rows, other_rows = slice(rows_a - CHUNK, rows_a), slice(0, rows_a - CHUNK)
    x_sem = load((r.x_hbm, r.x_in))
    moe_gain_sem = load((r.moe_gain_hbm, r.moe_gain))
    tail_sems = [
        load((r.value_hbm.at[tail_rows], r.value.at[tail_rows])),
        load((r.cgate_hbm.at[tail_rows], r.cgate.at[tail_rows])),
    ]
    gate_sems = [
        load((r.gate_hbm.at[0, :, cols], r.gate.at[:, cols]), (r.up_hbm.at[0, :, cols], r.up.at[:, cols]))
        for cols in gate_cols
    ]
    rest = [
        (r.value_hbm.at[other_rows], r.value.at[other_rows]),
        (r.cgate_hbm.at[other_rows], r.cgate.at[other_rows]),
        (r.sgate_hbm, r.sgate),
        (r.sup_hbm, r.sup),
        (r.taps_hbm, r.taps),
        (r.gain_hbm, r.gain),
        (r.shift_hbm, r.shift),
        (r.routes_hbm, r.routes),
        (r.route_weights_hbm, r.route_weights),
    ]
    rest_sems = [load(pair) for pair in rest]

    peers = [(place(b), q) for b in range(1, blocks)]
    peers += [(e, (q + k) % TP) for k in range(1, TP)]
    barrier = pltpu.get_barrier_semaphore()
    for peer in peers:
        pl.semaphore_signal(barrier, inc=1, device_id=peer, device_id_type=MESH)

    def chunk_of(i):
        return pl.multiple_of(i * CHUNK, CHUNK)

    def glu(i, carry):
        at = pl.ds(chunk_of(i), CHUNK)
        gated = r.value[at, :].astype(f32) * (1.0 / (1.0 + jnp.exp(-r.cgate[at, :].astype(f32))))
        padded[pl.ds(pl.multiple_of(i * CHUNK + edge, 8), CHUNK), :] = gated.astype(bf).astype(f32)
        return carry

    lane = lax.broadcasted_iota(jnp.int32, (CHUNK, 128), 1)

    def convolve(i, carry):
        start = chunk_of(i)
        at = pl.ds(start, CHUNK)
        sums, squares = jnp.zeros((CHUNK, 128), f32), jnp.zeros((CHUNK, 128), f32)
        for column in range(0, channels, 128):
            cols = slice(column, column + 128)
            window = padded[pl.ds(start, CHUNK + edge), cols]
            total = jnp.zeros((CHUNK, 128), f32)
            for b in range(8):
                size = CHUNK + (8 if b else 0)
                part = None
                for a in range(edge // 8 + 1):
                    j = 8 * a + b - lead
                    if 0 <= j < tap_count:
                        term = r.taps[j : j + 1, cols] * window[8 * a : 8 * a + size]
                        part = term if part is None else part + term
                if b:
                    part = pltpu.roll(part, size - b, 0)[:CHUNK]
                total = total + part
            r.filtered[at, cols] = total
            sums = sums + total
            squares = squares + total * total
        row_sum = jnp.sum(sums, axis=1, keepdims=True)
        row_squares = jnp.sum(squares, axis=1, keepdims=True)
        r.stats[at, :] = jnp.where(lane == 0, row_sum, jnp.where(lane == 1, row_squares, 0.0))
        return carry

    @phase
    def conv(first_chunk, last_chunk):
        lax.fori_loop(first_chunk, last_chunk, convolve, 0)

    @phase
    def halo():
        landed(r.halo, r.e_recv.at[0])
        padded[0:edge, :] = jnp.where(e == 0, 0.0, r.halo[...].astype(f32))

    @phase
    def send_stats():
        turned = r.stats[...].T
        lines = [turned[k : k + 1, slab(rows_a, spans, j)] for k in range(2) for j in range(spans)]
        r.rowsums[q] = jnp.concatenate(lines, axis=0)
        mine = r.rowsums.at[q]
        for k in range(1, TP):
            launch(mine, mine, r.m_send, r.m_recv.at[0], (e, (q + k) % TP))

    @phase
    def normalise():
        landed(r.rowsums.at[0 : TP - 1], r.m_recv.at[0])
        whole = (r.rowsums[0] + r.rowsums[1] + r.rowsums[2] + r.rowsums[3]) / (channels * TP)
        turned = jnp.concatenate([whole, jnp.zeros((SPAN - 2 * spans, SPAN), f32)], axis=0).T
        r.stats[0:SPAN, :] = turned
        for j in range(spans):

            def scale(i, carry):
                here = chunk_of(i)
                at = pl.ds(pl.multiple_of(here + j * SPAN, CHUNK), CHUNK)
                both = r.stats[pl.ds(here, CHUNK), :]
                mean, square = both[:, j : j + 1], both[:, spans + j : spans + j + 1]
                scaled = (r.filtered[at, :] - mean) * lax.rsqrt(square - mean * mean + 1e-05)
                chidden[q, at, :] = silu(scaled * r.gain[...] + r.shift[...]).astype(bf)
                return carry

            lax.fori_loop(0, SPAN // CHUNK, scale, 0)

    def send_conv(j):
        block = chidden.at[q, slab(rows_a, spans, j)]
        launch(block, block, r.c_send, r.ca_recv.at[j], across)
        launch(block, block, r.c_send, r.cs_recv.at[0], sister)

    @phase
    def relay_conv(j):
        block = chidden.at[far, slab(rows_a, spans, j)]
        landed(block, r.ca_recv.at[j])
        launch(block, block, r.c_send, r.cf_recv.at[j], sister)

    def conv_part(j, k):
        at = pl.ds(pl.multiple_of(k * channels, channels), channels)
        return dot(chidden[k, slab(rows_a, spans, j), :], r.cweight[at, :])

    @phase
    def project(j, base=None):
        at = slab(rows_a, spans, j)
        total = conv_part(j, q) + conv_part(j, side) + conv_part(j, far) if base is None else base + conv_part(j, far)
        landed(chidden.at[opposite, at], r.cf_recv.at[j])
        r.conv_out[at, :] = (total + conv_part(j, opposite)).astype(bf)

    def towards(src, slot, z_to):
        return copy(src, tokens.at[2 * slot, c], r.z_send, r.z_recv.at[slot - 1], (z_to * 2 + x, q))

    halves = [slab(rows, 2, i) for i in range(2)]

    @phase
    def pass_on(b, i=0, part=everything, condition=None):
        block = tokens.at[b, c, part]

        def along():
            (towards(block, 3, facing) if b == 2 else towards(block, b // 2, mate)).start()

        def act():
            landed(block, r.z_recv.at[b // 2 - 1] if b % 2 == 0 else r.t_recv.at[b // 2 + (1 if b > 1 else i)])
            if b % 2 == 0:
                if condition is inner:
                    along()
                elif condition is None:
                    pl.when(inner)(along)
                launch(block, tokens.at[b + 1, c, part], r.t_send, r.t_recv.at[b // 2 + 1], beside)
            launch(block, block, r.f_send, r.f_recv.at[b if b > 1 else i], sister)

        if condition is None:
            act()
        else:
            pl.when(condition)(act)

    @phase
    def swap_wait(b, i=0, part=everything):
        landed(tokens.at[b, 1 - c, part], r.f_recv.at[b if b > 1 else i])

    @phase
    def first(b, part, cols):
        def product(weight):
            return sum(dot(tokens[b, h, part, :], weight[h * half : (h + 1) * half, cols]) for h in range(2))

        hidden[b, q, part, cols] = (silu(product(r.gate)) * product(r.up)).astype(bf)
        block = hidden.at[b, q, part, cols]
        launch(block, block, r.h_send, r.y_recv.at[b], across)
        launch(block, block, r.h_send, r.p_recv.at[b], sister)

    def block_first(b):
        for t in range(2):
            first(b, everything, slab(units, 2, t))

    @phase
    def relay(b):
        block = hidden.at[b, far]
        landed(block, r.y_recv.at[b])
        launch(block, block, r.h_send, r.p_recv.at[b], sister)

    @phase
    def second_wait(b):
        landed(hidden.at[b, 0:2], r.p_recv.at[b])

    @phase
    def second(b):
        total = sum(dot(hidden[b, k], r.down[k * units : (k + 1) * units, :]) for k in range(TP))
        if b == 0:
            r.returned[0] = total.astype(bf)
        else:
            r.outgoing[b] = total.astype(bf)
            there = 2 * back[b // 2] + b % 2
            launch(r.outgoing.at[b], r.returned.at[there], r.r_send, r.r_recv.at[0], (place(b), q))

    def finish(b):
        second_wait(b)
        second(b)

    @phase
    def norm():
        loaded(x_sem, r.x_hbm, r.x_in)
        loaded(moe_gain_sem, r.moe_gain_hbm, r.moe_gain)
        for i in range(rows // 16):
            at = slice(i * 16, i * 16 + 16)
            v = r.x_in[at, :].astype(f32)
            scale = lax.rsqrt(jnp.mean(v * v, axis=1, keepdims=True) + 1e-06)
            normed = (v * scale * r.moe_gain[...]).astype(bf)
            tokens[0, 0, at, :] = normed[:, :half]
            tokens[0, 1, at, :] = normed[:, half:]

    @phase
    def tail_glu():
        loaded(tail_sems[0], r.value_hbm.at[tail_rows], r.value.at[tail_rows])
        loaded(tail_sems[1], r.cgate_hbm.at[tail_rows], r.cgate.at[tail_rows])
        glu(chunks - 1, 0)
        r.tail[...] = padded[rows_a:, :].astype(bf)

    @phase
    def meet():
        pl.semaphore_wait(barrier, len(peers))

    norm()
    tail_glu()
    meet()
    for i, part in enumerate(halves):
        launch(tokens.at[0, c, part], tokens.at[1, c, part], r.t_send, r.t_recv.at[i], beside)
    towards(tokens.at[0, c], 1, mate).start()
    pl.when(inner)(lambda: towards(tokens.at[0, c], 2, facing).start())
    launch(r.tail, r.halo, r.e_send, r.e_recv.at[0], ((e + 1) % blocks, q))

    for t, cols in enumerate(gate_cols):
        both = slab(units, PIECES // 2, 0)
        loaded(gate_sems[t], r.gate_hbm.at[0, :, both], r.gate.at[:, both])
        first(0, everything, cols)

    cweight_sem = load((r.cweight_hbm, r.cweight))
    down_sem = load((r.down_hbm.at[0], r.down))
    sdown_sem = load((r.sdown_hbm, r.sdown))

    @phase
    def glu_rest():
        for sem, pair in zip(rest_sems, rest, strict=True):
            loaded(sem, *pair)
        lax.fori_loop(0, chunks - 1, glu, 0)

    @phase
    def shared():
        def product(weight):
            return sum(dot(tokens[0, h], weight[h * half : (h + 1) * half, :]) for h in range(2))

        shidden[q] = (silu(product(r.sgate)) * product(r.sup)).astype(bf)
        launch(shidden.at[q], shidden.at[q], r.s_send, r.s_recv.at[0], across)
        launch(shidden.at[q], shidden.at[q], r.s_send, r.s_recv.at[1], sister)

    @phase
    def relay_shared():
        landed(shidden.at[far], r.s_recv.at[0])
        launch(shidden.at[far], shidden.at[far], r.s_send, r.s_recv.at[1], sister)

    @phase
    def shared_down():
        loaded(sdown_sem, r.sdown_hbm, r.sdown)
        landed(shidden.at[0:2], r.s_recv.at[1])
        share = shidden.shape[2]
        r.shared_sum[...] = sum(dot(shidden[k], r.sdown[k * share : (k + 1) * share, :]) for k in range(TP))

    @phase
    def combine():
        landed(r.returned.at[1:blocks], r.r_recv.at[0])
        routes, route_weights = r.routes[...], r.route_weights[...]
        lines = []
        for b in range(blocks):
            lines.append(jnp.sum(jnp.where(routes == place(b), route_weights, 0.0), axis=0, keepdims=True))
        lines.append(jnp.zeros((128 - blocks, rows), f32))
        weights = jnp.concatenate(lines, axis=0).T
        moe_sum = r.shared_sum[...]
        for b in range(blocks):
            moe_sum = moe_sum + weights[:, b : b + 1] * r.returned[b].astype(f32)
        r.out[...] = moe_sum.astype(bf)

    glu_rest()
    shared()
    conv(1, 4)
    pass_on(1, 0, halves[0])
    conv(4, 5)
    swap_wait(1, 0, halves[0])
    for t in range(2):
        first(1, halves[0], slab(units, 2, t))
    pass_on(1, 1, halves[1])
    pass_on(2)
    pass_on(4, condition=inner)
    conv(5, 6)
    swap_wait(1, 1, halves[1])
    for t in range(2):
        first(1, halves[1], slab(units, 2, t))
    swap_wait(2)
    block_first(2)
    relay(0)
    conv(6, 7)
    pass_on(4, condition=outer)
    conv(7, chunks)
    halo()
    conv(0, 1)
    send_stats()
    pass_on(6, condition=inner)
    pass_on(3)
    swap_wait(4)
    block_first(4)
    relay(1)
    relay_shared()
    loaded(down_sem, r.down_hbm.at[0], r.down)
    finish(0)
    swap_wait(3)
    block_first(3)
    pass_on(6, condition=outer)
    pass_on(5)
    finish(1)
    swap_wait(6)
    block_first(6)
    relay(2)
    swap_wait(5)
    block_first(5)
    finish(2)
    normalise()
    pass_on(7)
    swap_wait(7)
    block_first(7)
    for j in range(spans):
        send_conv(j)
    for b in (4, 3, 6, 5, 7):
        relay(b)
        if b == 7:
            shared_down()
        finish(b)
    loaded(cweight_sem, r.cweight_hbm, r.cweight)
    landed(chidden.at[side], r.cs_recv.at[0])
    last = spans - 1
    for j in range(last):
        relay_conv(j)
        if j:
            project(j - 1)
    r.partial[...] = conv_part(last, q) + conv_part(last, side)
    project(last - 1)
    relay_conv(last)
    combine()
    project(last, r.partial[...])

    @phase
    def drain():
        gone(hidden.at[:, 0:3], r.h_send)
        gone(r.outgoing.at[1:blocks], r.r_send)
        gone(tokens.at[0:depth, c], r.t_send)
        gone(tokens.at[1:blocks, c], r.f_send)
        pl.when(inner)(lambda: gone(tokens.at[0:5, c], r.z_send))
        pl.when(outer)(lambda: gone(tokens.at[0, c], r.z_send))
        gone(r.rowsums.at[0 : TP - 1], r.m_send)
        gone(shidden.at[0:3], r.s_send)
        gone(chidden.at[0:3], r.c_send)
        gone(r.tail, r.e_send)

    drain()


def hand_out(conv_done, done, conv_out, out, sems):
    copies = [
        pltpu.make_async_copy(src, dst, sems.at[i]) for i, (src, dst) in enumerate(((conv_done, conv_out), (done, out)))
    ]
    for cp in copies:
        cp.start()
    for cp in copies:
        cp.wait()


def fused(
    conv, moe_input, moe_gain, routes, route_weights, expert_gate, expert_up, expert_down, shared_gate, shared_up, shared_down
):
    value, cgate, taps, gain, shift, cweight = conv
    rows_a, channels = value.shape
    spans = rows_a // SPAN
    edge = -(-(taps.shape[0] - 1) // 8) * 8
    rows, width = moe_input.shape
    depth = lax.axis_size("ep") // 2
    blocks = 2 * depth
    units, columns = expert_gate.shape[2], expert_down.shape[2]
    bf, f32 = jnp.bfloat16, jnp.float32
    hbm = pl.BlockSpec(memory_space=pl.ANY)
    vmem = pl.BlockSpec(memory_space=pltpu.VMEM)

    def held(like):
        return pltpu.VMEM(like.shape, like.dtype)

    def dma(*shape):
        return pltpu.SemaphoreType.DMA(shape)

    gain, shift, moe_gain = gain.reshape(1, -1), shift.reshape(1, -1), moe_gain.reshape(1, -1)
    routes, route_weights = routes.T, route_weights.T
    operands = dict(
        x_hbm=moe_input,
        gate_hbm=expert_gate,
        up_hbm=expert_up,
        down_hbm=expert_down,
        sgate_hbm=shared_gate,
        sup_hbm=shared_up,
        sdown_hbm=shared_down,
        value_hbm=value,
        cgate_hbm=cgate,
        cweight_hbm=cweight,
        taps_hbm=taps,
        gain_hbm=gain,
        shift_hbm=shift,
        moe_gain_hbm=moe_gain,
        routes_hbm=routes,
        route_weights_hbm=route_weights,
    )
    outputs = dict(
        conv_out=jax.ShapeDtypeStruct((rows_a, cweight.shape[1]), bf),
        out=jax.ShapeDtypeStruct((rows, columns), bf),
    )
    scratch = dict(
        x_in=held(moe_input),
        sgate=held(shared_gate),
        sup=held(shared_up),
        sdown=held(shared_down),
        value=held(value),
        cgate=held(cgate),
        cweight=held(cweight),
        taps=held(taps),
        gain=held(gain),
        shift=held(shift),
        moe_gain=held(moe_gain),
        routes=held(routes),
        route_weights=held(route_weights),
        gate=pltpu.VMEM(expert_gate.shape[1:], bf),
        up=pltpu.VMEM(expert_up.shape[1:], bf),
        down=pltpu.VMEM(expert_down.shape[1:], bf),
        padded=pltpu.VMEM((rows_a + edge, channels), f32),
        filtered=pltpu.VMEM((rows_a, channels), f32),
        stats=pltpu.VMEM((rows_a, 128), f32),
        tail=pltpu.VMEM((edge, channels), bf),
        halo=pltpu.VMEM((edge, channels), bf),
        rowsums=pltpu.VMEM((TP, 2 * spans, SPAN), f32),
        chidden=pltpu.VMEM((TP, rows_a, channels), bf),
        partial=pltpu.VMEM((SPAN, cweight.shape[1]), f32),
        tokens=pltpu.VMEM((blocks, 2, rows, width // 2), bf),
        hidden=pltpu.VMEM((blocks, TP, rows, units), bf),
        returned=pltpu.VMEM((blocks, rows, columns), bf),
        outgoing=pltpu.VMEM((blocks, rows, columns), bf),
        shidden=pltpu.VMEM((TP, rows, shared_gate.shape[1]), bf),
        shared_sum=pltpu.VMEM((rows, columns), f32),
        load_sem=dma(PIECES + 16),
        e_send=dma(1),
        e_recv=dma(1),
        t_send=dma(1),
        t_recv=dma(depth + 1),
        f_send=dma(1),
        f_recv=dma(blocks),
        z_send=dma(1),
        z_recv=dma(depth - 1),
        h_send=dma(1),
        y_recv=dma(blocks),
        p_recv=dma(blocks),
        r_send=dma(1),
        r_recv=dma(1),
        m_send=dma(1),
        m_recv=dma(1),
        s_send=dma(1),
        s_recv=dma(2),
        c_send=dma(1),
        ca_recv=dma(spans),
        cs_recv=dma(1),
        cf_recv=dma(spans),
    )
    flops = 2 * blocks * rows * (2 * width * units + 4 * units * columns)
    results = pl.pallas_call(
        functools.partial(layer_kernel, depth, (*operands, *outputs, *scratch)),
        out_shape=tuple(pltpu.VMEM(out.shape, bf) for out in outputs.values()),
        in_specs=[hbm] * len(operands),
        out_specs=(vmem, vmem),
        scratch_shapes=list(scratch.values()),
        compiler_params=pltpu.CompilerParams(
            collective_id=0, has_side_effects=True, vmem_limit_bytes=58720256
        ),
        cost_estimate=pl.CostEstimate(flops=flops * 2, bytes_accessed=40_000_000, transcendentals=0),
    )(*operands.values())
    return pl.pallas_call(
        hand_out,
        out_shape=tuple(outputs.values()),
        in_specs=[vmem, vmem],
        out_specs=(hbm, hbm),
        scratch_shapes=[dma(2)],
        compiler_params=pltpu.CompilerParams(vmem_limit_bytes=4 * 1024 * 1024),
    )(*results)


def moe_general(normed, routes, route_weights, expert_gate, expert_up, expert_down, shared_gate, shared_up, shared_down):
    rows_b, per_row = routes.shape
    model_width = normed.shape[1]
    groups = lax.axis_size("ep")
    capacity = 2 * rows_b * per_row // groups
    flat_expert = routes.reshape(-1)
    owner_row = jnp.arange(rows_b * per_row, dtype=jnp.int32) // per_row
    expert_hits = (flat_expert[:, None] == jnp.arange(groups, dtype=jnp.int32)[None, :]).astype(
        jnp.int32
    )
    slot_rank = jnp.sum((jnp.cumsum(expert_hits, axis=0) - expert_hits) * expert_hits, axis=1)
    slot_index = flat_expert * capacity + slot_rank
    outgoing = (
        jnp.zeros((groups * capacity, model_width), jnp.bfloat16)
        .at[slot_index]
        .set(normed[owner_row])
    )
    outgoing = outgoing.reshape(groups, capacity, model_width)
    slot_share = capacity // lax.axis_size("tp")
    own_slots = lax.dynamic_slice_in_dim(outgoing, lax.axis_index("tp") * slot_share, slot_share, 1)
    partial_rows = lax.all_to_all(own_slots, "ep", split_axis=0, concat_axis=0, tiled=True)
    arrived = lax.all_gather(partial_rows, "tp", axis=1, tiled=True)
    arrived_rows = arrived.reshape(groups * capacity, model_width)
    gate_value = jnp.dot(arrived_rows, expert_gate[0], preferred_element_type=jnp.float32)
    upward = jnp.dot(arrived_rows, expert_up[0], preferred_element_type=jnp.float32)
    expert_hidden = (jax.nn.silu(gate_value) * upward).astype(jnp.bfloat16)
    shared_hidden = (
        jax.nn.silu(jnp.dot(normed, shared_gate, preferred_element_type=jnp.float32))
        * jnp.dot(normed, shared_up, preferred_element_type=jnp.float32)
    ).astype(jnp.bfloat16)
    columns = expert_down.shape[2]
    routed_sum = jnp.dot(
        lax.all_gather(expert_hidden, "tp", axis=1, tiled=True),
        expert_down[0],
        preferred_element_type=jnp.float32,
    )
    shared_sum = jnp.dot(
        lax.all_gather(shared_hidden, "tp", axis=1, tiled=True),
        shared_down,
        preferred_element_type=jnp.float32,
    )
    expert_out = routed_sum.astype(jnp.bfloat16).reshape(groups, capacity, columns)
    returned = lax.all_to_all(expert_out, "ep", split_axis=0, concat_axis=0, tiled=True).reshape(
        groups * capacity, columns
    )
    picked = returned[slot_index].astype(jnp.float32) * route_weights.reshape(-1)[:, None]
    moe_sum = jnp.sum(picked.reshape(rows_b, per_row, columns), axis=1) + shared_sum
    return moe_sum.astype(jnp.bfloat16)


def conv_general(conv_value, conv_gate, conv_taps, norm_gain, norm_shift, conv_out_weight):
    tap_count = conv_taps.shape[0]
    rows_a = conv_value.shape[0]
    glu_rows = (
        conv_value.astype(jnp.float32) * jax.nn.sigmoid(conv_gate.astype(jnp.float32))
    ).astype(jnp.bfloat16)
    before = from_behind(glu_rows[rows_a - (tap_count - 1) :], "ep", 1)
    padded = jnp.concatenate([before, glu_rows], axis=0)
    filtered = jnp.zeros(glu_rows.shape, jnp.float32)
    for offset in range(tap_count):
        filtered = filtered + conv_taps[offset] * padded[offset : offset + rows_a].astype(
            jnp.float32
        )
    row_total, squares = lax.psum(
        (jnp.sum(filtered, axis=1), jnp.sum(filtered * filtered, axis=1)), "tp"
    )
    channels = conv_out_weight.shape[0]
    row_mean = row_total / channels
    row_square = squares / channels
    scaled = (filtered - row_mean[:, None]) * lax.rsqrt(row_square - row_mean * row_mean + 1e-05)[
        :, None
    ]
    conv_hidden = jax.nn.silu(scaled * norm_gain + norm_shift).astype(jnp.bfloat16)
    conv_sum = jnp.dot(
        lax.all_gather(conv_hidden, "tp", axis=1, tiled=True),
        conv_out_weight,
        preferred_element_type=jnp.float32,
    )
    return conv_sum.astype(jnp.bfloat16)


def body(
    conv_value,
    conv_gate,
    conv_taps,
    norm_gain,
    norm_shift,
    conv_out_weight,
    moe_input,
    moe_gain,
    routes,
    route_weights,
    expert_gate,
    expert_up,
    expert_down,
    shared_gate,
    shared_up,
    shared_down,
):
    conv = (conv_value, conv_gate, conv_taps, norm_gain, norm_shift, conv_out_weight)
    moe = (routes, route_weights, expert_gate, expert_up, expert_down, shared_gate, shared_up, shared_down)
    if lax.axis_size("tp") == TP and lax.axis_size("ep") == 8 and moe_input.shape[0] == 128:
        return fused(conv, moe_input, moe_gain, *moe)
    inputs = moe_input.astype(jnp.float32)
    normed = (
        inputs * lax.rsqrt(jnp.mean(inputs * inputs, axis=1, keepdims=True) + 1e-06) * moe_gain
    ).astype(jnp.bfloat16)
    return (conv_general(*conv), moe_general(normed, *moe))


def solution(mesh):
    return jax.shard_map(
        body,
        mesh=mesh,
        in_specs=(
            P("ep", "tp"),
            P("ep", "tp"),
            P(None, "tp"),
            P("tp"),
            P("tp"),
            P(None, "tp"),
            P("ep", None),
            P(),
            P("ep", None),
            P("ep", None),
            P("ep", None, "tp"),
            P("ep", None, "tp"),
            P("ep", None, "tp"),
            P(None, "tp"),
            P(None, "tp"),
            P(None, "tp"),
        ),
        out_specs=(P("ep", "tp"), P("ep", "tp")),
        check_vma=False,
    )
```

```python
import functools
import types

import jax
import jax.numpy as jnp
from jax import lax
from jax.experimental import pallas as pl
from jax.experimental.pallas import tpu as pltpu
from jax.sharding import PartitionSpec as P

MESH = pl.DeviceIdType.MESH
CHUNK = 64
SPAN = 128
PIECES = 4
TP = 4


def from_behind(value, axis, steps):
    count = lax.axis_size(axis)
    initial, last = (max(0, -steps), min(count, count - steps))
    return lax.ppermute(value, axis, [(source, source + steps) for source in range(initial, last)])


def silu(v):
    return v / (1.0 + jnp.exp(-v))


def phase(step):
    def run(*args, **settings):
        with jax.named_scope(step.__name__):
            return step(*args, **settings)

    return run


def layer_kernel(depth, names, *refs):
    r = types.SimpleNamespace(**dict(zip(names, refs, strict=True)))
    e = lax.axis_index("ep")
    q = lax.axis_index("tp")
    z, x = e // 2, e % 2
    y, c = q // 2, q % 2
    side = y * 2 + (1 - c)
    far = (1 - y) * 2 + c
    opposite = (1 - y) * 2 + (1 - c)
    sister, across, beside = (e, side), (e, far), (z * 2 + (1 - x), q)
    blocks = 2 * depth
    bf, f32 = jnp.bfloat16, jnp.float32

    tokens, hidden, chidden, shidden, padded = r.tokens, r.hidden, r.chidden, r.shidden, r.padded
    rows, width = r.x_in.shape
    half = width // 2
    units = r.gate.shape[1]
    rows_a, channels = r.value.shape
    tap_count, edge = r.taps.shape[0], r.edges.shape[1]
    tail_out, halo_rows, passing = (r.edges.at[i] for i in range(3))
    lead = edge - (tap_count - 1)
    chunks = rows_a // CHUNK
    spans = rows_a // SPAN
    everything = slice(0, rows)

    upper = z // 2
    inside = (z + upper) % 2
    inner, outer = inside == 1, inside == 0
    mate = z + 1 - 2 * (z % 2)
    facing = depth - 1 - z
    origin = [z, mate, 2 - upper, 3 - 3 * upper]
    back = [0, 1, 3 - inside, 3 - inside]

    def place(b):
        return origin[b // 2] * 2 + (x if b % 2 == 0 else 1 - x)

    def slab(size, parts, i):
        return slice(i * size // parts, (i + 1) * size // parts)

    def dot(a, b):
        return jnp.dot(a, b, preferred_element_type=f32)

    def copy(src, dst, send, recv, device):
        return pltpu.make_async_remote_copy(
            src_ref=src, dst_ref=dst, send_sem=send.at[0], recv_sem=recv, device_id=device, device_id_type=MESH
        )

    def launch(*args):
        copy(*args).start()

    def landed(like, recv):
        copy(like, like, r.e_send, recv, beside).wait_recv()

    def gone(like, send):
        copy(like, like, send, r.e_recv.at[0], beside).wait_send()

    loads = []

    def load(*pairs):
        sem = r.load_sem.at[len(loads)]
        loads.append(sem)
        for src, dst in pairs:
            pltpu.make_async_copy(src, dst, sem).start()
        return sem

    def loaded(sem, src, dst):
        pltpu.make_async_copy(src, dst, sem).wait()

    gate_cols = [slab(units, PIECES, t) for t in range(PIECES)]
    tail_rows, other_rows = slice(rows_a - CHUNK, rows_a), slice(0, rows_a - CHUNK)
    x_sem = load((r.x_hbm, r.x_in))
    moe_gain_sem = load((r.moe_gain_hbm, r.moe_gain))
    tail_sems = [
        load((r.value_hbm.at[tail_rows], r.value.at[tail_rows])),
        load((r.cgate_hbm.at[tail_rows], r.cgate.at[tail_rows])),
    ]
    gate_sems = [
        load((r.gate_hbm.at[0, :, cols], r.gate.at[:, cols]), (r.up_hbm.at[0, :, cols], r.up.at[:, cols]))
        for cols in gate_cols
    ]
    rest = [
        (r.value_hbm.at[other_rows], r.value.at[other_rows]),
        (r.cgate_hbm.at[other_rows], r.cgate.at[other_rows]),
        (r.sgate_hbm, r.sgate),
        (r.sup_hbm, r.sup),
        (r.taps_hbm, r.taps),
        (r.gain_hbm, r.gain),
        (r.shift_hbm, r.shift),
        (r.routes_hbm, r.routes),
        (r.route_weights_hbm, r.route_weights),
    ]
    rest_sems = [load(pair) for pair in rest]

    peers = [beside, (mate * 2 + x, q)] + [(e, (q + k) % TP) for k in range(1, TP)]
    barrier = pltpu.get_barrier_semaphore()

    def greet(peer):
        pl.semaphore_signal(barrier, inc=1, device_id=peer, device_id_type=MESH)

    for peer in peers:
        greet(peer)
    pl.when(inner)(lambda: greet((facing * 2 + x, q)))

    def chunk_of(i):
        return pl.multiple_of(i * CHUNK, CHUNK)

    def glu(i, carry):
        at = pl.ds(chunk_of(i), CHUNK)
        gated = r.value[at, :].astype(f32) * (1.0 / (1.0 + jnp.exp(-r.cgate[at, :].astype(f32))))
        padded[pl.ds(pl.multiple_of(i * CHUNK + edge, 8), CHUNK), :] = gated.astype(bf).astype(f32)
        return carry

    lane = lax.broadcasted_iota(jnp.int32, (CHUNK, 128), 1)

    def convolve(i, carry):
        start = chunk_of(i)
        at = pl.ds(start, CHUNK)
        sums, squares = jnp.zeros((CHUNK, 128), f32), jnp.zeros((CHUNK, 128), f32)
        for column in range(0, channels, 128):
            cols = slice(column, column + 128)
            window = padded[pl.ds(start, CHUNK + edge), cols]
            total = jnp.zeros((CHUNK, 128), f32)
            for b in range(8):
                size = CHUNK + (8 if b else 0)
                part = None
                for a in range(edge // 8 + 1):
                    j = 8 * a + b - lead
                    if 0 <= j < tap_count:
                        term = r.taps[j : j + 1, cols] * window[8 * a : 8 * a + size]
                        part = term if part is None else part + term
                if b:
                    part = pltpu.roll(part, size - b, 0)[:CHUNK]
                total = total + part
            r.filtered[at, cols] = total
            sums = sums + total
            squares = squares + total * total
        row_sum = jnp.sum(sums, axis=1, keepdims=True)
        row_squares = jnp.sum(squares, axis=1, keepdims=True)
        r.stats[at, :] = jnp.where(lane == 0, row_sum, jnp.where(lane == 1, row_squares, 0.0))
        return carry

    @phase
    def conv(first_chunk, last_chunk):
        lax.fori_loop(first_chunk, last_chunk, convolve, 0)

    @phase
    def halo():
        @pl.when(e > 0)
        def _():
            landed(halo_rows, r.e_recv.at[0])
            padded[0:edge, :] = halo_rows[...].astype(f32)

        @pl.when(e == 0)
        def _():
            padded[0:edge, :] = jnp.zeros((edge, channels), f32)

    onward = (x == 0) & (z < depth - 1)

    @phase
    def send_edge():
        pl.when(x == 0)(lambda: launch(tail_out, halo_rows, r.e_send, r.e_recv.at[0], beside))
        pl.when(x == 1)(lambda: launch(tail_out, passing, r.e_send, r.e_recv.at[1], beside))

    @phase
    def relay_edge():
        pl.when(x == 0)(lambda: landed(passing, r.e_recv.at[1]))
        pl.when(onward)(lambda: launch(passing, halo_rows, r.e_send, r.e_recv.at[0], ((z + 1) * 2 + x, q)))

    @phase
    def send_stats():
        turned = r.stats[...].T
        lines = [turned[k : k + 1, slab(rows_a, spans, j)] for k in range(2) for j in range(spans)]
        r.rowsums[q] = jnp.concatenate(lines, axis=0)
        mine = r.rowsums.at[q]
        for k in range(1, TP):
            launch(mine, mine, r.m_send, r.m_recv.at[0], (e, (q + k) % TP))

    @phase
    def normalise():
        landed(r.rowsums.at[0 : TP - 1], r.m_recv.at[0])
        whole = (r.rowsums[0] + r.rowsums[1] + r.rowsums[2] + r.rowsums[3]) / (channels * TP)
        turned = jnp.concatenate([whole, jnp.zeros((SPAN - 2 * spans, SPAN), f32)], axis=0).T
        r.stats[0:SPAN, :] = turned
        for j in range(spans):

            def scale(i, carry):
                here = chunk_of(i)
                at = pl.ds(pl.multiple_of(here + j * SPAN, CHUNK), CHUNK)
                both = r.stats[pl.ds(here, CHUNK), :]
                mean, square = both[:, j : j + 1], both[:, spans + j : spans + j + 1]
                scaled = (r.filtered[at, :] - mean) * lax.rsqrt(square - mean * mean + 1e-05)
                chidden[q, at, :] = silu(scaled * r.gain[...] + r.shift[...]).astype(bf)
                return carry

            lax.fori_loop(0, SPAN // CHUNK, scale, 0)

    def send_conv(j):
        block = chidden.at[q, slab(rows_a, spans, j)]
        launch(block, block, r.c_send, r.ca_recv.at[j], across)
        launch(block, block, r.c_send, r.cs_recv.at[0], sister)

    @phase
    def relay_conv(j):
        block = chidden.at[far, slab(rows_a, spans, j)]
        landed(block, r.ca_recv.at[j])
        launch(block, block, r.c_send, r.cf_recv.at[j], sister)

    def conv_part(j, k):
        at = pl.ds(pl.multiple_of(k * channels, channels), channels)
        return dot(chidden[k, slab(rows_a, spans, j), :], r.cweight[at, :])

    @phase
    def project(j, base=None):
        at = slab(rows_a, spans, j)
        total = conv_part(j, q) + conv_part(j, side) + conv_part(j, far) if base is None else base + conv_part(j, far)
        landed(chidden.at[opposite, at], r.cf_recv.at[j])
        r.conv_out[at, :] = (total + conv_part(j, opposite)).astype(bf)

    def towards(src, slot, z_to):
        return copy(src, tokens.at[2 * slot, c], r.z_send, r.z_recv.at[slot - 1], (z_to * 2 + x, q))

    halves = [slab(rows, 2, i) for i in range(2)]

    @phase
    def pass_on(b, i=0, part=everything, condition=None):
        block = tokens.at[b, c, part]

        def along():
            (towards(block, 3, facing) if b == 2 else towards(block, b // 2, mate)).start()

        def act():
            landed(block, r.z_recv.at[b // 2 - 1] if b % 2 == 0 else r.t_recv.at[b // 2 + (1 if b > 1 else i)])
            if b % 2 == 0:
                if condition is inner:
                    along()
                elif condition is None:
                    pl.when(inner)(along)
                launch(block, tokens.at[b + 1, c, part], r.t_send, r.t_recv.at[b // 2 + 1], beside)
            launch(block, block, r.f_send, r.f_recv.at[b if b > 1 else i], sister)

        if condition is None:
            act()
        else:
            pl.when(condition)(act)

    @phase
    def swap_wait(b, i=0, part=everything):
        landed(tokens.at[b, 1 - c, part], r.f_recv.at[b if b > 1 else i])

    @phase
    def first(b, part, cols):
        def product(weight):
            return sum(dot(tokens[b, h, part, :], weight[h * half : (h + 1) * half, cols]) for h in range(2))

        hidden[b, q, part, cols] = (silu(product(r.gate)) * product(r.up)).astype(bf)
        block = hidden.at[b, q, part, cols]
        launch(block, block, r.h_send, r.y_recv.at[b], across)
        launch(block, block, r.h_send, r.p_recv.at[b], sister)

    def block_first(b):
        for t in range(2):
            first(b, everything, slab(units, 2, t))

    @phase
    def relay(b):
        block = hidden.at[b, far]
        landed(block, r.y_recv.at[b])
        launch(block, block, r.h_send, r.p_recv.at[b], sister)

    @phase
    def second_wait(b):
        landed(hidden.at[b, 0:2], r.p_recv.at[b])

    @phase
    def second(b):
        total = sum(dot(hidden[b, k], r.down[k * units : (k + 1) * units, :]) for k in range(TP))
        if b == 0:
            r.returned[0] = total.astype(bf)
        else:
            r.outgoing[b] = total.astype(bf)
            there = 2 * back[b // 2] + b % 2
            launch(r.outgoing.at[b], r.returned.at[there], r.r_send, r.r_recv.at[0], (place(b), q))

    def finish(b):
        second_wait(b)
        second(b)

    @phase
    def norm():
        loaded(x_sem, r.x_hbm, r.x_in)
        loaded(moe_gain_sem, r.moe_gain_hbm, r.moe_gain)
        for i in range(rows // 16):
            at = slice(i * 16, i * 16 + 16)
            v = r.x_in[at, :].astype(f32)
            scale = lax.rsqrt(jnp.mean(v * v, axis=1, keepdims=True) + 1e-06)
            normed = (v * scale * r.moe_gain[...]).astype(bf)
            tokens[0, 0, at, :] = normed[:, :half]
            tokens[0, 1, at, :] = normed[:, half:]

    @phase
    def tail_glu():
        loaded(tail_sems[0], r.value_hbm.at[tail_rows], r.value.at[tail_rows])
        loaded(tail_sems[1], r.cgate_hbm.at[tail_rows], r.cgate.at[tail_rows])
        glu(chunks - 1, 0)
        tail_out[...] = padded[rows_a:, :].astype(bf)

    @phase
    def meet():
        pl.when(inner)(lambda: pl.semaphore_wait(barrier, len(peers) + 1))
        pl.when(outer)(lambda: pl.semaphore_wait(barrier, len(peers)))

    norm()
    tail_glu()
    meet()
    for i, part in enumerate(halves):
        launch(tokens.at[0, c, part], tokens.at[1, c, part], r.t_send, r.t_recv.at[i], beside)
    towards(tokens.at[0, c], 1, mate).start()
    pl.when(inner)(lambda: towards(tokens.at[0, c], 2, facing).start())
    send_edge()

    for t, cols in enumerate(gate_cols):
        both = slab(units, PIECES // 2, 0)
        loaded(gate_sems[t], r.gate_hbm.at[0, :, both], r.gate.at[:, both])
        first(0, everything, cols)

    cweight_sem = load((r.cweight_hbm, r.cweight))
    down_sem = load((r.down_hbm.at[0], r.down))
    sdown_sem = load((r.sdown_hbm, r.sdown))

    @phase
    def glu_rest():
        for sem, pair in zip(rest_sems, rest, strict=True):
            loaded(sem, *pair)
        lax.fori_loop(0, chunks - 1, glu, 0)

    @phase
    def shared():
        def product(weight):
            return sum(dot(tokens[0, h], weight[h * half : (h + 1) * half, :]) for h in range(2))

        shidden[q] = (silu(product(r.sgate)) * product(r.sup)).astype(bf)
        launch(shidden.at[q], shidden.at[q], r.s_send, r.s_recv.at[0], across)
        launch(shidden.at[q], shidden.at[q], r.s_send, r.s_recv.at[1], sister)

    @phase
    def relay_shared():
        landed(shidden.at[far], r.s_recv.at[0])
        launch(shidden.at[far], shidden.at[far], r.s_send, r.s_recv.at[1], sister)

    @phase
    def shared_down():
        loaded(sdown_sem, r.sdown_hbm, r.sdown)
        landed(shidden.at[0:2], r.s_recv.at[1])
        share = shidden.shape[2]
        r.shared_sum[...] = sum(dot(shidden[k], r.sdown[k * share : (k + 1) * share, :]) for k in range(TP))

    @phase
    def combine():
        landed(r.returned.at[1:blocks], r.r_recv.at[0])
        routes, route_weights = r.routes[...], r.route_weights[...]
        lines = []
        for b in range(blocks):
            lines.append(jnp.sum(jnp.where(routes == place(b), route_weights, 0.0), axis=0, keepdims=True))
        lines.append(jnp.zeros((128 - blocks, rows), f32))
        weights = jnp.concatenate(lines, axis=0).T
        moe_sum = r.shared_sum[...]
        for b in range(blocks):
            moe_sum = moe_sum + weights[:, b : b + 1] * r.returned[b].astype(f32)
        r.out[...] = moe_sum.astype(bf)

    glu_rest()
    shared()
    conv(1, 4)
    pass_on(1, 0, halves[0])
    conv(4, 5)
    swap_wait(1, 0, halves[0])
    for t in range(2):
        first(1, halves[0], slab(units, 2, t))
    pass_on(1, 1, halves[1])
    pass_on(2)
    pass_on(4, condition=inner)
    relay_edge()
    conv(5, 6)
    swap_wait(1, 1, halves[1])
    for t in range(2):
        first(1, halves[1], slab(units, 2, t))
    swap_wait(2)
    block_first(2)
    relay(0)
    conv(6, 7)
    pass_on(6, condition=inner)
    pass_on(3)
    conv(7, chunks)
    swap_wait(3)
    block_first(3)
    pass_on(4, condition=outer)
    relay(1)
    relay_shared()
    loaded(down_sem, r.down_hbm.at[0], r.down)
    finish(0)
    swap_wait(4)
    block_first(4)
    halo()
    conv(0, 1)
    send_stats()
    pass_on(6, condition=outer)
    pass_on(5)
    finish(1)
    swap_wait(6)
    block_first(6)
    relay(2)
    finish(2)
    relay(3)
    finish(3)
    normalise()
    send_conv(0)
    relay(4)
    finish(4)
    pass_on(7)
    swap_wait(7)
    block_first(7)
    relay(6)
    finish(6)
    swap_wait(5)
    block_first(5)
    for j in range(1, spans):
        send_conv(j)
    shared_down()
    for b in (7, 5):
        relay(b)
        finish(b)
    loaded(cweight_sem, r.cweight_hbm, r.cweight)
    landed(chidden.at[side], r.cs_recv.at[0])
    last = spans - 1
    for j in range(last):
        relay_conv(j)
        if j:
            project(j - 1)
    r.partial[...] = conv_part(last, q) + conv_part(last, side)
    project(last - 1)
    relay_conv(last)
    combine()
    project(last, r.partial[...])

    @phase
    def drain():
        gone(hidden.at[:, 0:3], r.h_send)
        gone(r.outgoing.at[1:blocks], r.r_send)
        gone(tokens.at[0:depth, c], r.t_send)
        gone(tokens.at[1:blocks, c], r.f_send)
        pl.when(inner)(lambda: gone(tokens.at[0:5, c], r.z_send))
        pl.when(outer)(lambda: gone(tokens.at[0, c], r.z_send))
        gone(r.rowsums.at[0 : TP - 1], r.m_send)
        gone(shidden.at[0:3], r.s_send)
        gone(chidden.at[0:3], r.c_send)
        pl.when(onward)(lambda: gone(r.edges.at[0:2], r.e_send))
        pl.when(jnp.logical_not(onward))(lambda: gone(tail_out, r.e_send))

    drain()


def hand_out(conv_done, done, conv_out, out, sems):
    copies = [
        pltpu.make_async_copy(src, dst, sems.at[i]) for i, (src, dst) in enumerate(((conv_done, conv_out), (done, out)))
    ]
    for cp in copies:
        cp.start()
    for cp in copies:
        cp.wait()


def fused(
    conv, moe_input, moe_gain, routes, route_weights, expert_gate, expert_up, expert_down, shared_gate, shared_up, shared_down
):
    value, cgate, taps, gain, shift, cweight = conv
    rows_a, channels = value.shape
    spans = rows_a // SPAN
    edge = -(-(taps.shape[0] - 1) // 8) * 8
    rows, width = moe_input.shape
    depth = lax.axis_size("ep") // 2
    blocks = 2 * depth
    units, columns = expert_gate.shape[2], expert_down.shape[2]
    bf, f32 = jnp.bfloat16, jnp.float32
    hbm = pl.BlockSpec(memory_space=pl.ANY)
    vmem = pl.BlockSpec(memory_space=pltpu.VMEM)

    def held(like):
        return pltpu.VMEM(like.shape, like.dtype)

    def dma(*shape):
        return pltpu.SemaphoreType.DMA(shape)

    gain, shift, moe_gain = gain.reshape(1, -1), shift.reshape(1, -1), moe_gain.reshape(1, -1)
    routes, route_weights = routes.T, route_weights.T
    operands = dict(
        x_hbm=moe_input,
        gate_hbm=expert_gate,
        up_hbm=expert_up,
        down_hbm=expert_down,
        sgate_hbm=shared_gate,
        sup_hbm=shared_up,
        sdown_hbm=shared_down,
        value_hbm=value,
        cgate_hbm=cgate,
        cweight_hbm=cweight,
        taps_hbm=taps,
        gain_hbm=gain,
        shift_hbm=shift,
        moe_gain_hbm=moe_gain,
        routes_hbm=routes,
        route_weights_hbm=route_weights,
    )
    outputs = dict(
        conv_out=jax.ShapeDtypeStruct((rows_a, cweight.shape[1]), bf),
        out=jax.ShapeDtypeStruct((rows, columns), bf),
    )
    scratch = dict(
        x_in=held(moe_input),
        sgate=held(shared_gate),
        sup=held(shared_up),
        sdown=held(shared_down),
        value=held(value),
        cgate=held(cgate),
        cweight=held(cweight),
        taps=held(taps),
        gain=held(gain),
        shift=held(shift),
        moe_gain=held(moe_gain),
        routes=held(routes),
        route_weights=held(route_weights),
        gate=pltpu.VMEM(expert_gate.shape[1:], bf),
        up=pltpu.VMEM(expert_up.shape[1:], bf),
        down=pltpu.VMEM(expert_down.shape[1:], bf),
        padded=pltpu.VMEM((rows_a + edge, channels), f32),
        filtered=pltpu.VMEM((rows_a, channels), f32),
        stats=pltpu.VMEM((rows_a, 128), f32),
        edges=pltpu.VMEM((3, edge, channels), bf),
        rowsums=pltpu.VMEM((TP, 2 * spans, SPAN), f32),
        chidden=pltpu.VMEM((TP, rows_a, channels), bf),
        partial=pltpu.VMEM((SPAN, cweight.shape[1]), f32),
        tokens=pltpu.VMEM((blocks, 2, rows, width // 2), bf),
        hidden=pltpu.VMEM((blocks, TP, rows, units), bf),
        returned=pltpu.VMEM((blocks, rows, columns), bf),
        outgoing=pltpu.VMEM((blocks, rows, columns), bf),
        shidden=pltpu.VMEM((TP, rows, shared_gate.shape[1]), bf),
        shared_sum=pltpu.VMEM((rows, columns), f32),
        load_sem=dma(PIECES + 16),
        e_send=dma(1),
        e_recv=dma(2),
        t_send=dma(1),
        t_recv=dma(depth + 1),
        f_send=dma(1),
        f_recv=dma(blocks),
        z_send=dma(1),
        z_recv=dma(depth - 1),
        h_send=dma(1),
        y_recv=dma(blocks),
        p_recv=dma(blocks),
        r_send=dma(1),
        r_recv=dma(1),
        m_send=dma(1),
        m_recv=dma(1),
        s_send=dma(1),
        s_recv=dma(2),
        c_send=dma(1),
        ca_recv=dma(spans),
        cs_recv=dma(1),
        cf_recv=dma(spans),
    )
    flops = 2 * blocks * rows * (2 * width * units + 4 * units * columns)
    results = pl.pallas_call(
        functools.partial(layer_kernel, depth, (*operands, *outputs, *scratch)),
        out_shape=tuple(pltpu.VMEM(out.shape, bf) for out in outputs.values()),
        in_specs=[hbm] * len(operands),
        out_specs=(vmem, vmem),
        scratch_shapes=list(scratch.values()),
        compiler_params=pltpu.CompilerParams(
            collective_id=0, has_side_effects=True, vmem_limit_bytes=58720256
        ),
        cost_estimate=pl.CostEstimate(flops=flops * 2, bytes_accessed=40_000_000, transcendentals=0),
    )(*operands.values())
    return pl.pallas_call(
        hand_out,
        out_shape=tuple(outputs.values()),
        in_specs=[vmem, vmem],
        out_specs=(hbm, hbm),
        scratch_shapes=[dma(2)],
        compiler_params=pltpu.CompilerParams(vmem_limit_bytes=4 * 1024 * 1024),
    )(*results)


def moe_general(normed, routes, route_weights, expert_gate, expert_up, expert_down, shared_gate, shared_up, shared_down):
    rows_b, per_row = routes.shape
    model_width = normed.shape[1]
    groups = lax.axis_size("ep")
    capacity = 2 * rows_b * per_row // groups
    flat_expert = routes.reshape(-1)
    owner_row = jnp.arange(rows_b * per_row, dtype=jnp.int32) // per_row
    expert_hits = (flat_expert[:, None] == jnp.arange(groups, dtype=jnp.int32)[None, :]).astype(
        jnp.int32
    )
    slot_rank = jnp.sum((jnp.cumsum(expert_hits, axis=0) - expert_hits) * expert_hits, axis=1)
    slot_index = flat_expert * capacity + slot_rank
    outgoing = (
        jnp.zeros((groups * capacity, model_width), jnp.bfloat16)
        .at[slot_index]
        .set(normed[owner_row])
    )
    outgoing = outgoing.reshape(groups, capacity, model_width)
    slot_share = capacity // lax.axis_size("tp")
    own_slots = lax.dynamic_slice_in_dim(outgoing, lax.axis_index("tp") * slot_share, slot_share, 1)
    partial_rows = lax.all_to_all(own_slots, "ep", split_axis=0, concat_axis=0, tiled=True)
    arrived = lax.all_gather(partial_rows, "tp", axis=1, tiled=True)
    arrived_rows = arrived.reshape(groups * capacity, model_width)
    gate_value = jnp.dot(arrived_rows, expert_gate[0], preferred_element_type=jnp.float32)
    upward = jnp.dot(arrived_rows, expert_up[0], preferred_element_type=jnp.float32)
    expert_hidden = (jax.nn.silu(gate_value) * upward).astype(jnp.bfloat16)
    shared_hidden = (
        jax.nn.silu(jnp.dot(normed, shared_gate, preferred_element_type=jnp.float32))
        * jnp.dot(normed, shared_up, preferred_element_type=jnp.float32)
    ).astype(jnp.bfloat16)
    columns = expert_down.shape[2]
    routed_sum = jnp.dot(
        lax.all_gather(expert_hidden, "tp", axis=1, tiled=True),
        expert_down[0],
        preferred_element_type=jnp.float32,
    )
    shared_sum = jnp.dot(
        lax.all_gather(shared_hidden, "tp", axis=1, tiled=True),
        shared_down,
        preferred_element_type=jnp.float32,
    )
    expert_out = routed_sum.astype(jnp.bfloat16).reshape(groups, capacity, columns)
    returned = lax.all_to_all(expert_out, "ep", split_axis=0, concat_axis=0, tiled=True).reshape(
        groups * capacity, columns
    )
    picked = returned[slot_index].astype(jnp.float32) * route_weights.reshape(-1)[:, None]
    moe_sum = jnp.sum(picked.reshape(rows_b, per_row, columns), axis=1) + shared_sum
    return moe_sum.astype(jnp.bfloat16)


def conv_general(conv_value, conv_gate, conv_taps, norm_gain, norm_shift, conv_out_weight):
    tap_count = conv_taps.shape[0]
    rows_a = conv_value.shape[0]
    glu_rows = (
        conv_value.astype(jnp.float32) * jax.nn.sigmoid(conv_gate.astype(jnp.float32))
    ).astype(jnp.bfloat16)
    before = from_behind(glu_rows[rows_a - (tap_count - 1) :], "ep", 1)
    padded = jnp.concatenate([before, glu_rows], axis=0)
    filtered = jnp.zeros(glu_rows.shape, jnp.float32)
    for offset in range(tap_count):
        filtered = filtered + conv_taps[offset] * padded[offset : offset + rows_a].astype(
            jnp.float32
        )
    row_total, squares = lax.psum(
        (jnp.sum(filtered, axis=1), jnp.sum(filtered * filtered, axis=1)), "tp"
    )
    channels = conv_out_weight.shape[0]
    row_mean = row_total / channels
    row_square = squares / channels
    scaled = (filtered - row_mean[:, None]) * lax.rsqrt(row_square - row_mean * row_mean + 1e-05)[
        :, None
    ]
    conv_hidden = jax.nn.silu(scaled * norm_gain + norm_shift).astype(jnp.bfloat16)
    conv_sum = jnp.dot(
        lax.all_gather(conv_hidden, "tp", axis=1, tiled=True),
        conv_out_weight,
        preferred_element_type=jnp.float32,
    )
    return conv_sum.astype(jnp.bfloat16)


def body(
    conv_value,
    conv_gate,
    conv_taps,
    norm_gain,
    norm_shift,
    conv_out_weight,
    moe_input,
    moe_gain,
    routes,
    route_weights,
    expert_gate,
    expert_up,
    expert_down,
    shared_gate,
    shared_up,
    shared_down,
):
    conv = (conv_value, conv_gate, conv_taps, norm_gain, norm_shift, conv_out_weight)
    moe = (routes, route_weights, expert_gate, expert_up, expert_down, shared_gate, shared_up, shared_down)
    if lax.axis_size("tp") == TP and lax.axis_size("ep") == 8 and moe_input.shape[0] == 128:
        return fused(conv, moe_input, moe_gain, *moe)
    inputs = moe_input.astype(jnp.float32)
    normed = (
        inputs * lax.rsqrt(jnp.mean(inputs * inputs, axis=1, keepdims=True) + 1e-06) * moe_gain
    ).astype(jnp.bfloat16)
    return (conv_general(*conv), moe_general(normed, *moe))


def solution(mesh):
    return jax.shard_map(
        body,
        mesh=mesh,
        in_specs=(
            P("ep", "tp"),
            P("ep", "tp"),
            P(None, "tp"),
            P("tp"),
            P("tp"),
            P(None, "tp"),
            P("ep", None),
            P(),
            P("ep", None),
            P("ep", None),
            P("ep", None, "tp"),
            P("ep", None, "tp"),
            P("ep", None, "tp"),
            P(None, "tp"),
            P(None, "tp"),
            P(None, "tp"),
        ),
        out_specs=(P("ep", "tp"), P("ep", "tp")),
        check_vma=False,
    )
```

```python
import functools
import types

import jax
import jax.numpy as jnp
from jax import lax
from jax.experimental import pallas as pl
from jax.experimental.pallas import tpu as pltpu
from jax.sharding import PartitionSpec as P

MESH = pl.DeviceIdType.MESH
CHUNK = 64
SPAN = 128
PIECES = 4
TP = 4


def from_behind(value, axis, steps):
    count = lax.axis_size(axis)
    initial, last = (max(0, -steps), min(count, count - steps))
    return lax.ppermute(value, axis, [(source, source + steps) for source in range(initial, last)])


def silu(v):
    return v / (1.0 + jnp.exp(-v))


def phase(step):
    def run(*args, **settings):
        with jax.named_scope(step.__name__):
            return step(*args, **settings)

    return run


def layer_kernel(depth, names, *refs):
    r = types.SimpleNamespace(**dict(zip(names, refs, strict=True)))
    e = lax.axis_index("ep")
    q = lax.axis_index("tp")
    z, x = e // 2, e % 2
    y, c = q // 2, q % 2
    side = y * 2 + (1 - c)
    far = (1 - y) * 2 + c
    opposite = (1 - y) * 2 + (1 - c)
    sister, across, beside = (e, side), (e, far), (z * 2 + (1 - x), q)
    blocks = 2 * depth
    bf, f32 = jnp.bfloat16, jnp.float32

    tokens, hidden, chidden, shidden, padded = r.tokens, r.hidden, r.chidden, r.shidden, r.padded
    rows, width = r.x_in.shape
    half = width // 2
    units = r.gate.shape[1]
    rows_a, channels = r.value.shape
    tap_count, edge = r.taps.shape[0], r.edges.shape[1]
    tail_out, halo_rows, passing = (r.edges.at[i] for i in range(3))
    lead = edge - (tap_count - 1)
    chunks = rows_a // CHUNK
    spans = rows_a // SPAN
    everything = slice(0, rows)

    upper = z // 2
    inside = (z + upper) % 2
    inner, outer = inside == 1, inside == 0
    mate = z + 1 - 2 * (z % 2)
    facing = depth - 1 - z
    origin = [z, mate, 2 - upper, 3 - 3 * upper]
    back = [0, 1, 3 - inside, 3 - inside]

    def place(b):
        return origin[b // 2] * 2 + (x if b % 2 == 0 else 1 - x)

    def slab(size, parts, i):
        return slice(i * size // parts, (i + 1) * size // parts)

    def dot(a, b):
        return jnp.dot(a, b, preferred_element_type=f32)

    def copy(src, dst, send, recv, device):
        return pltpu.make_async_remote_copy(
            src_ref=src, dst_ref=dst, send_sem=send.at[0], recv_sem=recv, device_id=device, device_id_type=MESH
        )

    def launch(*args):
        copy(*args).start()

    def landed(like, recv):
        copy(like, like, r.e_send, recv, beside).wait_recv()

    def gone(like, send):
        copy(like, like, send, r.e_recv.at[0], beside).wait_send()

    loads = []

    def load(*pairs):
        sem = r.load_sem.at[len(loads)]
        loads.append(sem)
        for src, dst in pairs:
            pltpu.make_async_copy(src, dst, sem).start()
        return sem

    def loaded(sem, src, dst):
        pltpu.make_async_copy(src, dst, sem).wait()

    gate_cols = [slab(units, PIECES, t) for t in range(PIECES)]
    tail_rows, other_rows = slice(rows_a - CHUNK, rows_a), slice(0, rows_a - CHUNK)
    x_sem = load((r.x_hbm, r.x_in))
    moe_gain_sem = load((r.moe_gain_hbm, r.moe_gain))
    tail_sems = [
        load((r.value_hbm.at[tail_rows], r.value.at[tail_rows])),
        load((r.cgate_hbm.at[tail_rows], r.cgate.at[tail_rows])),
    ]
    gate_sems = [
        load((r.gate_hbm.at[0, :, cols], r.gate.at[:, cols]), (r.up_hbm.at[0, :, cols], r.up.at[:, cols]))
        for cols in gate_cols
    ]
    rest = [
        (r.value_hbm.at[other_rows], r.value.at[other_rows]),
        (r.cgate_hbm.at[other_rows], r.cgate.at[other_rows]),
        (r.sgate_hbm, r.sgate),
        (r.sup_hbm, r.sup),
        (r.taps_hbm, r.taps),
        (r.gain_hbm, r.gain),
        (r.shift_hbm, r.shift),
        (r.routes_hbm, r.routes),
        (r.route_weights_hbm, r.route_weights),
    ]
    rest_sems = [load(pair) for pair in rest]

    peers = [beside, (mate * 2 + x, q)] + [(e, (q + k) % TP) for k in range(1, TP)]
    barrier = pltpu.get_barrier_semaphore()

    def greet(peer):
        pl.semaphore_signal(barrier, inc=1, device_id=peer, device_id_type=MESH)

    for peer in peers:
        greet(peer)
    pl.when(inner)(lambda: greet((facing * 2 + x, q)))

    def chunk_of(i):
        return pl.multiple_of(i * CHUNK, CHUNK)

    def glu(i, carry):
        at = pl.ds(chunk_of(i), CHUNK)
        gated = r.value[at, :].astype(f32) * (1.0 / (1.0 + jnp.exp(-r.cgate[at, :].astype(f32))))
        padded[pl.ds(pl.multiple_of(i * CHUNK + edge, 8), CHUNK), :] = gated.astype(bf).astype(f32)
        return carry

    lane = lax.broadcasted_iota(jnp.int32, (CHUNK, 128), 1)

    def convolve(i, carry):
        start = chunk_of(i)
        at = pl.ds(start, CHUNK)
        sums, squares = jnp.zeros((CHUNK, 128), f32), jnp.zeros((CHUNK, 128), f32)
        for column in range(0, channels, 128):
            cols = slice(column, column + 128)
            window = padded[pl.ds(start, CHUNK + edge), cols]
            total = jnp.zeros((CHUNK, 128), f32)
            for b in range(8):
                size = CHUNK + (8 if b else 0)
                part = None
                for a in range(edge // 8 + 1):
                    j = 8 * a + b - lead
                    if 0 <= j < tap_count:
                        term = r.taps[j : j + 1, cols] * window[8 * a : 8 * a + size]
                        part = term if part is None else part + term
                if b:
                    part = pltpu.roll(part, size - b, 0)[:CHUNK]
                total = total + part
            r.filtered[at, cols] = total
            sums = sums + total
            squares = squares + total * total
        row_sum = jnp.sum(sums, axis=1, keepdims=True)
        row_squares = jnp.sum(squares, axis=1, keepdims=True)
        r.stats[at, :] = jnp.where(lane == 0, row_sum, jnp.where(lane == 1, row_squares, 0.0))
        return carry

    @phase
    def conv(first_chunk, last_chunk):
        lax.fori_loop(first_chunk, last_chunk, convolve, 0)

    @phase
    def halo():
        @pl.when(e > 0)
        def _():
            landed(halo_rows, r.e_recv.at[0])
            padded[0:edge, :] = halo_rows[...].astype(f32)

        @pl.when(e == 0)
        def _():
            padded[0:edge, :] = jnp.zeros((edge, channels), f32)

    onward = (x == 0) & (z < depth - 1)

    @phase
    def send_edge():
        pl.when(x == 0)(lambda: launch(tail_out, halo_rows, r.e_send, r.e_recv.at[0], beside))
        pl.when(x == 1)(lambda: launch(tail_out, passing, r.e_send, r.e_recv.at[1], beside))

    @phase
    def relay_edge():
        pl.when(x == 0)(lambda: landed(passing, r.e_recv.at[1]))
        pl.when(onward)(lambda: launch(passing, halo_rows, r.e_send, r.e_recv.at[0], ((z + 1) * 2 + x, q)))

    @phase
    def send_stats():
        turned = r.stats[...].T
        lines = [turned[k : k + 1, slab(rows_a, spans, j)] for k in range(2) for j in range(spans)]
        r.rowsums[q] = jnp.concatenate(lines, axis=0)
        mine = r.rowsums.at[q]
        for k in range(1, TP):
            launch(mine, mine, r.m_send, r.m_recv.at[0], (e, (q + k) % TP))

    @phase
    def normalise():
        landed(r.rowsums.at[0 : TP - 1], r.m_recv.at[0])
        whole = (r.rowsums[0] + r.rowsums[1] + r.rowsums[2] + r.rowsums[3]) / (channels * TP)
        turned = jnp.concatenate([whole, jnp.zeros((SPAN - 2 * spans, SPAN), f32)], axis=0).T
        r.stats[0:SPAN, :] = turned
        for j in range(spans):

            def scale(i, carry):
                here = chunk_of(i)
                at = pl.ds(pl.multiple_of(here + j * SPAN, CHUNK), CHUNK)
                both = r.stats[pl.ds(here, CHUNK), :]
                mean, square = both[:, j : j + 1], both[:, spans + j : spans + j + 1]
                scaled = (r.filtered[at, :] - mean) * lax.rsqrt(square - mean * mean + 1e-05)
                chidden[q, at, :] = silu(scaled * r.gain[...] + r.shift[...]).astype(bf)
                return carry

            lax.fori_loop(0, SPAN // CHUNK, scale, 0)

    def send_conv(j):
        block = chidden.at[q, slab(rows_a, spans, j)]
        launch(block, block, r.c_send, r.ca_recv.at[j], across)
        launch(block, block, r.c_send, r.cs_recv.at[0], sister)

    @phase
    def relay_conv(j):
        block = chidden.at[far, slab(rows_a, spans, j)]
        landed(block, r.ca_recv.at[j])
        launch(block, block, r.c_send, r.cf_recv.at[j], sister)

    def conv_part(j, k):
        at = pl.ds(pl.multiple_of(k * channels, channels), channels)
        return dot(chidden[k, slab(rows_a, spans, j), :], r.cweight[at, :])

    @phase
    def project(j, base=None):
        at = slab(rows_a, spans, j)
        total = conv_part(j, q) + conv_part(j, side) + conv_part(j, far) if base is None else base + conv_part(j, far)
        landed(chidden.at[opposite, at], r.cf_recv.at[j])
        r.conv_out[at, :] = (total + conv_part(j, opposite)).astype(bf)

    def towards(src, slot, z_to):
        return copy(src, tokens.at[2 * slot, c], r.z_send, r.z_recv.at[slot - 1], (z_to * 2 + x, q))

    halves = [slab(rows, 2, i) for i in range(2)]

    @phase
    def pass_on(b, i=0, part=everything, condition=None):
        block = tokens.at[b, c, part]

        def along():
            (towards(block, 3, facing) if b == 2 else towards(block, b // 2, mate)).start()

        def act():
            landed(block, r.z_recv.at[b // 2 - 1] if b % 2 == 0 else r.t_recv.at[b // 2 + (1 if b > 1 else i)])
            if b % 2 == 0:
                if condition is inner:
                    along()
                elif condition is None:
                    pl.when(inner)(along)
                launch(block, tokens.at[b + 1, c, part], r.t_send, r.t_recv.at[b // 2 + 1], beside)
            launch(block, block, r.f_send, r.f_recv.at[b if b > 1 else i], sister)

        if condition is None:
            act()
        else:
            pl.when(condition)(act)

    @phase
    def swap_wait(b, i=0, part=everything):
        landed(tokens.at[b, 1 - c, part], r.f_recv.at[b if b > 1 else i])

    @phase
    def first(b, part, cols):
        def product(weight):
            return sum(dot(tokens[b, h, part, :], weight[h * half : (h + 1) * half, cols]) for h in range(2))

        hidden[b, q, part, cols] = (silu(product(r.gate)) * product(r.up)).astype(bf)
        block = hidden.at[b, q, part, cols]
        launch(block, block, r.h_send, r.y_recv.at[b], across)
        launch(block, block, r.h_send, r.p_recv.at[b], sister)

    def block_first(b):
        for t in range(2):
            first(b, everything, slab(units, 2, t))

    @phase
    def relay(b):
        block = hidden.at[b, far]
        landed(block, r.y_recv.at[b])
        launch(block, block, r.h_send, r.p_recv.at[b], sister)

    @phase
    def second_wait(b):
        landed(hidden.at[b, 0:2], r.p_recv.at[b])

    @phase
    def second(b):
        total = sum(dot(hidden[b, k], r.down[k * units : (k + 1) * units, :]) for k in range(TP))
        if b == 0:
            r.returned[0] = total.astype(bf)
        else:
            r.outgoing[b] = total.astype(bf)
            there = 2 * back[b // 2] + b % 2
            launch(r.outgoing.at[b], r.returned.at[there], r.r_send, r.r_recv.at[0], (place(b), q))

    def finish(b):
        second_wait(b)
        second(b)

    @phase
    def norm():
        loaded(x_sem, r.x_hbm, r.x_in)
        loaded(moe_gain_sem, r.moe_gain_hbm, r.moe_gain)
        for i in range(rows // 16):
            at = slice(i * 16, i * 16 + 16)
            v = r.x_in[at, :].astype(f32)
            scale = lax.rsqrt(jnp.mean(v * v, axis=1, keepdims=True) + 1e-06)
            normed = (v * scale * r.moe_gain[...]).astype(bf)
            tokens[0, 0, at, :] = normed[:, :half]
            tokens[0, 1, at, :] = normed[:, half:]

    @phase
    def tail_glu():
        loaded(tail_sems[0], r.value_hbm.at[tail_rows], r.value.at[tail_rows])
        loaded(tail_sems[1], r.cgate_hbm.at[tail_rows], r.cgate.at[tail_rows])
        glu(chunks - 1, 0)
        tail_out[...] = padded[rows_a:, :].astype(bf)

    @phase
    def meet():
        pl.when(inner)(lambda: pl.semaphore_wait(barrier, len(peers) + 1))
        pl.when(outer)(lambda: pl.semaphore_wait(barrier, len(peers)))

    norm()
    tail_glu()
    meet()
    for i, part in enumerate(halves):
        launch(tokens.at[0, c, part], tokens.at[1, c, part], r.t_send, r.t_recv.at[i], beside)
    towards(tokens.at[0, c], 1, mate).start()
    pl.when(inner)(lambda: towards(tokens.at[0, c], 2, facing).start())
    send_edge()

    for t, cols in enumerate(gate_cols):
        both = slab(units, PIECES // 2, 0)
        loaded(gate_sems[t], r.gate_hbm.at[0, :, both], r.gate.at[:, both])
        first(0, everything, cols)

    cweight_sem = load((r.cweight_hbm, r.cweight))
    down_sem = load((r.down_hbm.at[0], r.down))
    sdown_sem = load((r.sdown_hbm, r.sdown))

    @phase
    def glu_rest():
        for sem, pair in zip(rest_sems, rest, strict=True):
            loaded(sem, *pair)
        lax.fori_loop(0, chunks - 1, glu, 0)

    @phase
    def shared():
        def product(weight):
            return sum(dot(tokens[0, h], weight[h * half : (h + 1) * half, :]) for h in range(2))

        shidden[q] = (silu(product(r.sgate)) * product(r.sup)).astype(bf)
        launch(shidden.at[q], shidden.at[q], r.s_send, r.s_recv.at[0], across)
        launch(shidden.at[q], shidden.at[q], r.s_send, r.s_recv.at[1], sister)

    @phase
    def relay_shared():
        landed(shidden.at[far], r.s_recv.at[0])
        launch(shidden.at[far], shidden.at[far], r.s_send, r.s_recv.at[1], sister)

    @phase
    def shared_down():
        loaded(sdown_sem, r.sdown_hbm, r.sdown)
        landed(shidden.at[0:2], r.s_recv.at[1])
        share = shidden.shape[2]
        r.shared_sum[...] = sum(dot(shidden[k], r.sdown[k * share : (k + 1) * share, :]) for k in range(TP))

    @phase
    def weigh():
        routes, route_weights = r.routes[...], r.route_weights[...]
        lines = []
        for b in range(blocks):
            lines.append(jnp.sum(jnp.where(routes == place(b), route_weights, 0.0), axis=0, keepdims=True))
        lines.append(jnp.zeros((128 - blocks, rows), f32))
        r.weights[...] = jnp.concatenate(lines, axis=0).T
        r.shared_sum[...] += r.weights[:, 0:1] * r.returned[0].astype(f32)

    @phase
    def combine():
        landed(r.returned.at[1:blocks], r.r_recv.at[0])
        weights = r.weights[...]
        moe_sum = r.shared_sum[...]
        for b in range(1, blocks):
            moe_sum = moe_sum + weights[:, b : b + 1] * r.returned[b].astype(f32)
        r.out[...] = moe_sum.astype(bf)

    small_first = [slab(units, PIECES, 0), slab(units, PIECES, 1), slab(units, 2, 1)]
    glu_rest()
    shared()
    conv(1, 4)
    pass_on(1, 0, halves[0])
    conv(4, 5)
    swap_wait(1, 0, halves[0])
    for cols in small_first:
        first(1, halves[0], cols)
    pass_on(1, 1, halves[1])
    pass_on(2)
    pass_on(4, condition=inner)
    relay_edge()
    conv(5, 6)
    swap_wait(1, 1, halves[1])
    for cols in small_first:
        first(1, halves[1], cols)
    swap_wait(2)
    block_first(2)
    relay(0)
    conv(6, 7)
    pass_on(6, condition=inner)
    pass_on(3)
    conv(7, chunks)
    swap_wait(3)
    block_first(3)
    pass_on(4, condition=outer)
    relay(1)
    relay_shared()
    loaded(down_sem, r.down_hbm.at[0], r.down)
    finish(0)
    swap_wait(4)
    block_first(4)
    halo()
    conv(0, 1)
    send_stats()
    pass_on(6, condition=outer)
    pass_on(5)
    finish(1)
    swap_wait(6)
    block_first(6)
    relay(2)
    finish(2)
    relay(3)
    finish(3)
    normalise()
    send_conv(0)
    relay(4)
    finish(4)
    pass_on(7)
    swap_wait(7)
    block_first(7)
    relay(6)
    finish(6)
    swap_wait(5)
    block_first(5)
    for j in range(1, spans):
        send_conv(j)
    shared_down()
    weigh()
    for b in (7, 5):
        relay(b)
        finish(b)
    loaded(cweight_sem, r.cweight_hbm, r.cweight)
    landed(chidden.at[side], r.cs_recv.at[0])
    last = spans - 1
    for j in range(last):
        relay_conv(j)
        if j:
            project(j - 1)
    r.partial[...] = conv_part(last, q) + conv_part(last, side)
    project(last - 1)
    relay_conv(last)
    combine()
    project(last, r.partial[...])

    @phase
    def drain():
        gone(hidden.at[:, 0:3], r.h_send)
        gone(r.outgoing.at[1:blocks], r.r_send)
        gone(tokens.at[0:depth, c], r.t_send)
        gone(tokens.at[1:blocks, c], r.f_send)
        pl.when(inner)(lambda: gone(tokens.at[0:5, c], r.z_send))
        pl.when(outer)(lambda: gone(tokens.at[0, c], r.z_send))
        gone(r.rowsums.at[0 : TP - 1], r.m_send)
        gone(shidden.at[0:3], r.s_send)
        gone(chidden.at[0:3], r.c_send)
        pl.when(onward)(lambda: gone(r.edges.at[0:2], r.e_send))
        pl.when(jnp.logical_not(onward))(lambda: gone(tail_out, r.e_send))

    drain()


def hand_out(conv_done, done, conv_out, out, sems):
    copies = [
        pltpu.make_async_copy(src, dst, sems.at[i]) for i, (src, dst) in enumerate(((conv_done, conv_out), (done, out)))
    ]
    for cp in copies:
        cp.start()
    for cp in copies:
        cp.wait()


def fused(
    conv, moe_input, moe_gain, routes, route_weights, expert_gate, expert_up, expert_down, shared_gate, shared_up, shared_down
):
    value, cgate, taps, gain, shift, cweight = conv
    rows_a, channels = value.shape
    spans = rows_a // SPAN
    edge = -(-(taps.shape[0] - 1) // 8) * 8
    rows, width = moe_input.shape
    depth = lax.axis_size("ep") // 2
    blocks = 2 * depth
    units, columns = expert_gate.shape[2], expert_down.shape[2]
    bf, f32 = jnp.bfloat16, jnp.float32
    hbm = pl.BlockSpec(memory_space=pl.ANY)
    vmem = pl.BlockSpec(memory_space=pltpu.VMEM)

    def held(like):
        return pltpu.VMEM(like.shape, like.dtype)

    def dma(*shape):
        return pltpu.SemaphoreType.DMA(shape)

    gain, shift, moe_gain = gain.reshape(1, -1), shift.reshape(1, -1), moe_gain.reshape(1, -1)
    routes, route_weights = routes.T, route_weights.T
    operands = dict(
        x_hbm=moe_input,
        gate_hbm=expert_gate,
        up_hbm=expert_up,
        down_hbm=expert_down,
        sgate_hbm=shared_gate,
        sup_hbm=shared_up,
        sdown_hbm=shared_down,
        value_hbm=value,
        cgate_hbm=cgate,
        cweight_hbm=cweight,
        taps_hbm=taps,
        gain_hbm=gain,
        shift_hbm=shift,
        moe_gain_hbm=moe_gain,
        routes_hbm=routes,
        route_weights_hbm=route_weights,
    )
    outputs = dict(
        conv_out=jax.ShapeDtypeStruct((rows_a, cweight.shape[1]), bf),
        out=jax.ShapeDtypeStruct((rows, columns), bf),
    )
    scratch = dict(
        x_in=held(moe_input),
        sgate=held(shared_gate),
        sup=held(shared_up),
        sdown=held(shared_down),
        value=held(value),
        cgate=held(cgate),
        cweight=held(cweight),
        taps=held(taps),
        gain=held(gain),
        shift=held(shift),
        moe_gain=held(moe_gain),
        routes=held(routes),
        route_weights=held(route_weights),
        gate=pltpu.VMEM(expert_gate.shape[1:], bf),
        up=pltpu.VMEM(expert_up.shape[1:], bf),
        down=pltpu.VMEM(expert_down.shape[1:], bf),
        padded=pltpu.VMEM((rows_a + edge, channels), f32),
        filtered=pltpu.VMEM((rows_a, channels), f32),
        stats=pltpu.VMEM((rows_a, 128), f32),
        edges=pltpu.VMEM((3, edge, channels), bf),
        rowsums=pltpu.VMEM((TP, 2 * spans, SPAN), f32),
        chidden=pltpu.VMEM((TP, rows_a, channels), bf),
        partial=pltpu.VMEM((SPAN, cweight.shape[1]), f32),
        tokens=pltpu.VMEM((blocks, 2, rows, width // 2), bf),
        hidden=pltpu.VMEM((blocks, TP, rows, units), bf),
        returned=pltpu.VMEM((blocks, rows, columns), bf),
        outgoing=pltpu.VMEM((blocks, rows, columns), bf),
        shidden=pltpu.VMEM((TP, rows, shared_gate.shape[1]), bf),
        shared_sum=pltpu.VMEM((rows, columns), f32),
        weights=pltpu.VMEM((rows, 128), f32),
        load_sem=dma(PIECES + 16),
        e_send=dma(1),
        e_recv=dma(2),
        t_send=dma(1),
        t_recv=dma(depth + 1),
        f_send=dma(1),
        f_recv=dma(blocks),
        z_send=dma(1),
        z_recv=dma(depth - 1),
        h_send=dma(1),
        y_recv=dma(blocks),
        p_recv=dma(blocks),
        r_send=dma(1),
        r_recv=dma(1),
        m_send=dma(1),
        m_recv=dma(1),
        s_send=dma(1),
        s_recv=dma(2),
        c_send=dma(1),
        ca_recv=dma(spans),
        cs_recv=dma(1),
        cf_recv=dma(spans),
    )
    flops = 2 * blocks * rows * (2 * width * units + 4 * units * columns)
    results = pl.pallas_call(
        functools.partial(layer_kernel, depth, (*operands, *outputs, *scratch)),
        out_shape=tuple(pltpu.VMEM(out.shape, bf) for out in outputs.values()),
        in_specs=[hbm] * len(operands),
        out_specs=(vmem, vmem),
        scratch_shapes=list(scratch.values()),
        compiler_params=pltpu.CompilerParams(
            collective_id=0, has_side_effects=True, vmem_limit_bytes=58720256
        ),
        cost_estimate=pl.CostEstimate(flops=flops * 2, bytes_accessed=40_000_000, transcendentals=0),
    )(*operands.values())
    return pl.pallas_call(
        hand_out,
        out_shape=tuple(outputs.values()),
        in_specs=[vmem, vmem],
        out_specs=(hbm, hbm),
        scratch_shapes=[dma(2)],
        compiler_params=pltpu.CompilerParams(vmem_limit_bytes=4 * 1024 * 1024),
    )(*results)


def moe_general(normed, routes, route_weights, expert_gate, expert_up, expert_down, shared_gate, shared_up, shared_down):
    rows_b, per_row = routes.shape
    model_width = normed.shape[1]
    groups = lax.axis_size("ep")
    capacity = 2 * rows_b * per_row // groups
    flat_expert = routes.reshape(-1)
    owner_row = jnp.arange(rows_b * per_row, dtype=jnp.int32) // per_row
    expert_hits = (flat_expert[:, None] == jnp.arange(groups, dtype=jnp.int32)[None, :]).astype(
        jnp.int32
    )
    slot_rank = jnp.sum((jnp.cumsum(expert_hits, axis=0) - expert_hits) * expert_hits, axis=1)
    slot_index = flat_expert * capacity + slot_rank
    outgoing = (
        jnp.zeros((groups * capacity, model_width), jnp.bfloat16)
        .at[slot_index]
        .set(normed[owner_row])
    )
    outgoing = outgoing.reshape(groups, capacity, model_width)
    slot_share = capacity // lax.axis_size("tp")
    own_slots = lax.dynamic_slice_in_dim(outgoing, lax.axis_index("tp") * slot_share, slot_share, 1)
    partial_rows = lax.all_to_all(own_slots, "ep", split_axis=0, concat_axis=0, tiled=True)
    arrived = lax.all_gather(partial_rows, "tp", axis=1, tiled=True)
    arrived_rows = arrived.reshape(groups * capacity, model_width)
    gate_value = jnp.dot(arrived_rows, expert_gate[0], preferred_element_type=jnp.float32)
    upward = jnp.dot(arrived_rows, expert_up[0], preferred_element_type=jnp.float32)
    expert_hidden = (jax.nn.silu(gate_value) * upward).astype(jnp.bfloat16)
    shared_hidden = (
        jax.nn.silu(jnp.dot(normed, shared_gate, preferred_element_type=jnp.float32))
        * jnp.dot(normed, shared_up, preferred_element_type=jnp.float32)
    ).astype(jnp.bfloat16)
    columns = expert_down.shape[2]
    routed_sum = jnp.dot(
        lax.all_gather(expert_hidden, "tp", axis=1, tiled=True),
        expert_down[0],
        preferred_element_type=jnp.float32,
    )
    shared_sum = jnp.dot(
        lax.all_gather(shared_hidden, "tp", axis=1, tiled=True),
        shared_down,
        preferred_element_type=jnp.float32,
    )
    expert_out = routed_sum.astype(jnp.bfloat16).reshape(groups, capacity, columns)
    returned = lax.all_to_all(expert_out, "ep", split_axis=0, concat_axis=0, tiled=True).reshape(
        groups * capacity, columns
    )
    picked = returned[slot_index].astype(jnp.float32) * route_weights.reshape(-1)[:, None]
    moe_sum = jnp.sum(picked.reshape(rows_b, per_row, columns), axis=1) + shared_sum
    return moe_sum.astype(jnp.bfloat16)


def conv_general(conv_value, conv_gate, conv_taps, norm_gain, norm_shift, conv_out_weight):
    tap_count = conv_taps.shape[0]
    rows_a = conv_value.shape[0]
    glu_rows = (
        conv_value.astype(jnp.float32) * jax.nn.sigmoid(conv_gate.astype(jnp.float32))
    ).astype(jnp.bfloat16)
    before = from_behind(glu_rows[rows_a - (tap_count - 1) :], "ep", 1)
    padded = jnp.concatenate([before, glu_rows], axis=0)
    filtered = jnp.zeros(glu_rows.shape, jnp.float32)
    for offset in range(tap_count):
        filtered = filtered + conv_taps[offset] * padded[offset : offset + rows_a].astype(
            jnp.float32
        )
    row_total, squares = lax.psum(
        (jnp.sum(filtered, axis=1), jnp.sum(filtered * filtered, axis=1)), "tp"
    )
    channels = conv_out_weight.shape[0]
    row_mean = row_total / channels
    row_square = squares / channels
    scaled = (filtered - row_mean[:, None]) * lax.rsqrt(row_square - row_mean * row_mean + 1e-05)[
        :, None
    ]
    conv_hidden = jax.nn.silu(scaled * norm_gain + norm_shift).astype(jnp.bfloat16)
    conv_sum = jnp.dot(
        lax.all_gather(conv_hidden, "tp", axis=1, tiled=True),
        conv_out_weight,
        preferred_element_type=jnp.float32,
    )
    return conv_sum.astype(jnp.bfloat16)


def body(
    conv_value,
    conv_gate,
    conv_taps,
    norm_gain,
    norm_shift,
    conv_out_weight,
    moe_input,
    moe_gain,
    routes,
    route_weights,
    expert_gate,
    expert_up,
    expert_down,
    shared_gate,
    shared_up,
    shared_down,
):
    conv = (conv_value, conv_gate, conv_taps, norm_gain, norm_shift, conv_out_weight)
    moe = (routes, route_weights, expert_gate, expert_up, expert_down, shared_gate, shared_up, shared_down)
    if lax.axis_size("tp") == TP and lax.axis_size("ep") == 8 and moe_input.shape[0] == 128:
        return fused(conv, moe_input, moe_gain, *moe)
    inputs = moe_input.astype(jnp.float32)
    normed = (
        inputs * lax.rsqrt(jnp.mean(inputs * inputs, axis=1, keepdims=True) + 1e-06) * moe_gain
    ).astype(jnp.bfloat16)
    return (conv_general(*conv), moe_general(normed, *moe))


def solution(mesh):
    return jax.shard_map(
        body,
        mesh=mesh,
        in_specs=(
            P("ep", "tp"),
            P("ep", "tp"),
            P(None, "tp"),
            P("tp"),
            P("tp"),
            P(None, "tp"),
            P("ep", None),
            P(),
            P("ep", None),
            P("ep", None),
            P("ep", None, "tp"),
            P("ep", None, "tp"),
            P("ep", None, "tp"),
            P(None, "tp"),
            P(None, "tp"),
            P(None, "tp"),
        ),
        out_specs=(P("ep", "tp"), P("ep", "tp")),
        check_vma=False,
    )
```
